32 devices in a mesh: sp: 8 (over z, x), tp: 4 (over y, core).
Axes of the slice: x: 2, y: 2, z: 4, core: 2. Of those that a mesh axis runs over, the one named last changes fastest.
Arguments:
- residual: bfloat16 [8192, 2048], P('sp'), may hold values from -6 to 6
- query: bfloat16 [8192, 1024], P('sp', 'tp'), may hold values from -6 to 6
- key: bfloat16 [8192, 256], P('sp', 'tp'), may hold values from -6 to 6
- value: bfloat16 [8192, 256], P('sp', 'tp'), may hold values from -6 to 6
- sink: float32 [16], P('tp'), may hold values from 3 to 9
- norm_gain: float32 [2048], replicated, may hold values from 0.1 to 1.9
- w_out: bfloat16 [1024, 2048], P('tp'), may hold values from -1.5 to 1.5
- w_gate: bfloat16 [2048, 4096], P('sp', 'tp'), may hold values from -0.125 to 0.125
- w_value: bfloat16 [2048, 4096], P('sp', 'tp'), may hold values from -0.125 to 0.125
- conv_gate: bfloat16 [3, 4096], P(None, 'tp'), may hold values from -3 to 3
- conv_value: bfloat16 [3, 4096], P(None, 'tp'), may hold values from -3 to 3
- w_down: bfloat16 [4096, 2048], P('tp', 'sp'), may hold values from -0.09375 to 0.09375
Outputs:
- layer_out: bfloat16 [8192, 2048], P(('sp', 'tp'))
The draws below stay inside these ranges and needn't reach their ends.
All inputs are finite; a program needn't handle non-finite values.
Results may differ from the reference program's by a relative error of at most 0.015.
Values may be sent and summed in bfloat16 or wider, within the bound.
A program may use at most 128 MiB of HBM per device.

```python
import jax
import jax.numpy as jnp
from jax import lax

D = 2048
FF = 4096
HEADS = 16
KV_HEADS = 4
HD = 64
WINDOW = 128
TOKENS = 8192
N_TP = 4


def draw_key(key, part):
    base = jax.random.fold_in(key, 11)
    shape = (TOKENS, KV_HEADS * HD)
    return jnp.clip(jax.random.normal(jax.random.fold_in(base, 1), shape, jnp.float32), -6.0, 6.0).astype(jnp.bfloat16)


def draw_query(key, part):
    base = jax.random.fold_in(key, 11)
    shape = (TOKENS, HEADS * HD)
    return jnp.clip(jax.random.normal(jax.random.fold_in(base, 2), shape, jnp.float32), -6.0, 6.0).astype(jnp.bfloat16)


def steps_of(key, shape, split, smallest, top_value):
    level = 1.0
    for dim, shards_of in split:
        heights = jax.random.uniform(jax.random.fold_in(jax.random.fold_in(key, 6), dim), (shards_of,), jnp.float32, smallest / len(split), top_value / len(split))
        level = level * jnp.repeat(jnp.exp(heights), shape[dim] // shards_of).reshape((-1,) + (1,) * (len(shape) - 1 - dim))
    return level


def bell_draw(stream_key, dims, scale, most, shards=(), held_as=jnp.bfloat16):
    level = steps_of(stream_key, dims, shards, -0.22, 0.18) if shards else 1.0
    array = jax.random.normal(stream_key, dims, jnp.float32) * scale * level
    return jnp.minimum(jnp.maximum(array, -most), most).astype(held_as)


def setup_inputs(seed: int = 0) -> dict:
    key_of = jax.random.split(jax.random.key(seed), 13)
    residual = bell_draw(key_of[0], (TOKENS, D), 1.0, 6.0, ((0, 8),))
    query = draw_query(jax.random.fold_in(key_of[12], 71), 0)
    key = draw_key(jax.random.fold_in(key_of[12], 71), 0)
    value = bell_draw(key_of[3], (TOKENS, KV_HEADS * HD), 1.0, 6.0, ((0, 8), (1, 4)))
    sink = jnp.clip(3.0 + 6.0 * jax.random.uniform(key_of[4], (HEADS,), jnp.float32) ** steps_of(key_of[4], (HEADS,), ((0, 4),), -0.2, 0.2), 3.0, 9.0)
    norm_gain = jnp.clip(1.0 + 0.18 * jax.random.normal(key_of[5], (D,), jnp.float32), 0.1, 1.9)
    w_out = bell_draw(key_of[6], (HEADS * HD, D), (HD // 4) ** -0.5, 1.5, ((0, 4),))
    w_gate = bell_draw(key_of[7], (D, FF), D ** -0.5, 0.125, ((0, 8), (1, 4)))
    w_value = bell_draw(key_of[8], (D, FF), D ** -0.5, 0.125, ((0, 8), (1, 4)))
    conv_gate = bell_draw(key_of[9], (3, FF), 0.577, 3.0, ((1, 4),))
    conv_value = bell_draw(key_of[10], (3, FF), 0.577, 3.0, ((1, 4),))
    w_down = bell_draw(key_of[11], (FF, D), FF ** -0.5, 0.09375, ((0, 4), (1, 8)))
    return {"residual": residual, "query": query, "key": key, "value": value, "sink": sink, "norm_gain": norm_gain, "w_out": w_out, "w_gate": w_gate, "w_value": w_value, "conv_gate": conv_gate, "conv_value": conv_value, "w_down": w_down}


THETA = 10000.0
EPS = 1e-06

def rotate(field, positions):
    count = field.shape[0]
    parts = field.astype(jnp.float32).reshape(count, -1, HD)
    inverse = 1.0 / THETA ** (jnp.arange(0, HD, 2, dtype=jnp.float32) / HD)
    angle = positions[:, None] * inverse[None, :]
    cosine = jnp.cos(angle)[:, None, :]
    sine = jnp.sin(angle)[:, None, :]
    first = parts[..., :HD // 2]
    second = parts[..., HD // 2:]
    turned = jnp.concatenate([first * cosine - second * sine, second * cosine + first * sine], axis=-1)
    return turned.reshape(count, -1).astype(jnp.bfloat16)

def band_attention(queries, keys, values, sinks, start, total):
    count = queries.shape[0]
    blocks = count // WINDOW
    kv_local = keys.shape[1] // HD
    group = queries.shape[1] // (kv_local * HD)
    query_blocks = queries.astype(jnp.float32).reshape(blocks, WINDOW, kv_local, group, HD)
    key_band = jnp.concatenate([keys[i * WINDOW:i * WINDOW + count].reshape(blocks, WINDOW, kv_local, HD) for i in range(3)], axis=1).astype(jnp.float32)
    value_band = jnp.concatenate([values[i * WINDOW:i * WINDOW + count].reshape(blocks, WINDOW, kv_local, HD) for i in range(3)], axis=1).astype(jnp.float32)
    scores = jnp.einsum('nqkgd,njkd->nkgqj', query_blocks, key_band) * HD ** (-0.5)
    block_ids = jnp.arange(blocks, dtype=jnp.int32)[:, None]
    query_pos = start + block_ids * WINDOW + jnp.arange(WINDOW, dtype=jnp.int32)[None, :]
    key_pos = start - WINDOW + block_ids * WINDOW + jnp.arange(3 * WINDOW, dtype=jnp.int32)[None, :]
    valid = (key_pos[:, None, :] >= 0) & (key_pos[:, None, :] < total) & (jnp.abs(query_pos[:, :, None] - key_pos[:, None, :]) <= WINDOW)
    scores = jnp.where(valid[:, None, None], scores, -1e+30)
    sink_col = sinks.astype(jnp.float32).reshape(1, kv_local, group, 1, 1)
    top = jnp.maximum(lax.optimization_barrier(jnp.max(scores, axis=-1, keepdims=True)), sink_col)
    weights = jnp.exp(scores - top)
    denom = lax.optimization_barrier(jnp.sum(weights, axis=-1, keepdims=True)) + jnp.exp(sink_col - top)
    probs = (weights / denom).astype(jnp.bfloat16)
    out = jnp.einsum('nkgqj,njkd->nqkgd', probs.astype(jnp.float32), value_band)
    return out.reshape(count, kv_local * group * HD).astype(jnp.bfloat16)

def rmsnorm(field, gain):
    wide = field.astype(jnp.float32)
    scale = lax.rsqrt(lax.optimization_barrier(jnp.mean(wide * wide, axis=-1, keepdims=True)) + EPS)
    return (wide * scale * gain).astype(jnp.bfloat16)

def block_sum(left, right, pieces):
    width = left.shape[1] // pieces
    summed = jnp.zeros((left.shape[0], right.shape[1]), jnp.float32)
    for index in range(pieces):
        term = jnp.dot(left[:, index * width:(index + 1) * width], right[index * width:(index + 1) * width], preferred_element_type=jnp.float32)
        rounded = lax.optimization_barrier(term.astype(jnp.bfloat16))
        summed = summed + rounded.astype(jnp.float32)
    return summed

def reference(residual, query, key, value, sink, norm_gain, w_out, w_gate, w_value, conv_gate, conv_value, w_down):
    total = query.shape[0]
    kv_heads = key.shape[1] // HD
    group = query.shape[1] // key.shape[1]
    positions = jnp.arange(total, dtype=jnp.float32)
    turned_query = rotate(query, positions)
    turned_key = rotate(key, positions)
    pad = ((WINDOW, WINDOW), (0, 0))
    keys_ext = jnp.pad(turned_key, pad)
    values_ext = jnp.pad(value, pad)
    query_heads = turned_query.reshape(total, kv_heads, group * HD).transpose(1, 0, 2)
    key_heads = keys_ext.reshape(total + 2 * WINDOW, kv_heads, HD).transpose(1, 0, 2)
    value_heads = values_ext.reshape(total + 2 * WINDOW, kv_heads, HD).transpose(1, 0, 2)
    sink_heads = sink.reshape(kv_heads, group)

    def one_head(args):
        return band_attention(args[0], args[1], args[2], args[3], 0, total)
    outs = lax.map(one_head, (query_heads, key_heads, value_heads, sink_heads))
    attended = outs.transpose(1, 0, 2).reshape(total, -1)
    mix = block_sum(attended, w_out, N_TP)
    mid = (residual.astype(jnp.float32) + mix).astype(jnp.bfloat16)
    normed = rmsnorm(mid, norm_gain)
    gate_up = jnp.dot(normed, w_gate, preferred_element_type=jnp.float32).astype(jnp.bfloat16)
    value_up = jnp.dot(normed, w_value, preferred_element_type=jnp.float32).astype(jnp.bfloat16)

    def convolve(field, taps):
        padded = jnp.pad(field, ((1, 1), (0, 0))).astype(jnp.float32)
        taps = taps.astype(jnp.float32)
        return padded[:-2] * taps[0] + padded[1:-1] * taps[1] + padded[2:] * taps[2]
    gate_conv = convolve(gate_up, conv_gate)
    value_conv = convolve(value_up, conv_value)
    hidden = (jax.nn.silu(gate_conv) * value_conv).astype(jnp.bfloat16)
    ffn = block_sum(hidden, w_down, N_TP)
    return (mid.astype(jnp.float32) + ffn).astype(jnp.bfloat16)
```

```python
import functools

import jax
import jax.numpy as jnp
import numpy as np
from jax import lax
from jax.experimental import pallas as pl
from jax.experimental.pallas import tpu as pltpu
from jax.sharding import PartitionSpec as P

HD = 64
WINDOW = 128


THETA = 10000.0
EPS = 1e-06


def extended(block, sides, width):
    for axis, dim in sides:
        count = lax.axis_size(axis)
        forward = [(i, i + 1) for i in range(count - 1)]
        backward = [(target, source) for source, target in forward]
        low = lax.ppermute(
            lax.slice_in_dim(block, block.shape[dim] - width, None, axis=dim), axis, forward
        )
        high = lax.ppermute(lax.slice_in_dim(block, 0, width, axis=dim), axis, backward)
        block = jnp.concatenate([low, block, high], axis=dim)
    return block


def rotate(field, positions):
    count = field.shape[0]
    parts = field.astype(jnp.float32).reshape(count, -1, HD)
    inverse = 1.0 / THETA ** (jnp.arange(0, HD, 2, dtype=jnp.float32) / HD)
    angle = positions[:, None] * inverse[None, :]
    cosine = jnp.cos(angle)[:, None, :]
    sine = jnp.sin(angle)[:, None, :]
    first = parts[..., : HD // 2]
    second = parts[..., HD // 2 :]
    turned = jnp.concatenate(
        [first * cosine - second * sine, second * cosine + first * sine], axis=-1
    )
    return turned.reshape(count, -1).astype(jnp.bfloat16)


def band_attention(queries, keys, values, sinks, start, total):
    count = queries.shape[0]
    blocks = count // WINDOW
    kv_local = keys.shape[1] // HD
    group = queries.shape[1] // (kv_local * HD)
    query_blocks = queries.reshape(blocks, WINDOW, kv_local, group, HD)
    key_band = jnp.concatenate(
        [
            keys[i * WINDOW : i * WINDOW + count].reshape(blocks, WINDOW, kv_local, HD)
            for i in range(3)
        ],
        axis=1,
    )
    value_band = jnp.concatenate(
        [
            values[i * WINDOW : i * WINDOW + count].reshape(blocks, WINDOW, kv_local, HD)
            for i in range(3)
        ],
        axis=1,
    )
    scores = jnp.einsum(
        "nqkgd,njkd->nkgqj", query_blocks, key_band, preferred_element_type=jnp.float32
    ) * HD ** (-0.5)
    block_ids = jnp.arange(blocks, dtype=jnp.int32)[:, None]
    query_pos = start + block_ids * WINDOW + jnp.arange(WINDOW, dtype=jnp.int32)[None, :]
    key_pos = start - WINDOW + block_ids * WINDOW + jnp.arange(3 * WINDOW, dtype=jnp.int32)[None, :]
    valid = (
        (key_pos[:, None, :] >= 0)
        & (key_pos[:, None, :] < total)
        & (jnp.abs(query_pos[:, :, None] - key_pos[:, None, :]) <= WINDOW)
    )
    scores = jnp.where(valid[:, None, None], scores, -1e30)
    sink_col = sinks.reshape(1, kv_local, group, 1, 1)
    top = jnp.maximum(jnp.max(scores, axis=-1, keepdims=True), sink_col)
    weights = jnp.exp(scores - top)
    denom = jnp.sum(weights, axis=-1, keepdims=True) + jnp.exp(sink_col - top)
    probs = (weights / denom).astype(jnp.bfloat16)
    out = jnp.einsum("nkgqj,njkd->nqkgd", probs, value_band, preferred_element_type=jnp.float32)
    return out.reshape(count, kv_local * group * HD).astype(jnp.bfloat16)


def rmsnorm(field, gain):
    wide = field.astype(jnp.float32)
    scale = lax.rsqrt(jnp.mean(wide * wide, axis=-1, keepdims=True) + EPS)
    return (wide * scale * gain).astype(jnp.bfloat16)


def plain_shards(
    residual,
    query,
    key,
    value,
    sink,
    norm_gain,
    w_out,
    w_gate,
    w_value,
    conv_gate,
    conv_value,
    w_down,
):
    tok_rows = query.shape[0]
    offset = lax.axis_index("sp") * tok_rows
    total = tok_rows * lax.axis_size("sp")
    share = tok_rows // lax.axis_size("tp")
    tp_index = lax.axis_index("tp")
    positions = (offset + jnp.arange(tok_rows, dtype=jnp.int32)).astype(jnp.float32)
    turned_query = rotate(query, positions)
    turned_key = rotate(key, positions)
    key_width = key.shape[1]
    band = jnp.concatenate([turned_key, value], axis=1)
    edged = extended(band, (("sp", 0),), WINDOW)
    attended = band_attention(
        turned_query, edged[:, :key_width], edged[:, key_width:], sink, offset, total
    )
    partial_value = jnp.dot(attended, w_out, preferred_element_type=jnp.float32)
    mix_full = lax.psum(partial_value.astype(jnp.bfloat16), "tp").astype(jnp.float32)
    mid_full = (residual.astype(jnp.float32) + mix_full).astype(jnp.bfloat16)
    normed = rmsnorm(mid_full, norm_gain)
    mid_rows = lax.dynamic_slice_in_dim(mid_full, tp_index * share, share, 0)
    gate_full, value_full = (
        lax.all_gather(w_gate, "sp", axis=0, tiled=True),
        lax.all_gather(w_value, "sp", axis=0, tiled=True),
    )
    gate_up = jnp.dot(normed, gate_full, preferred_element_type=jnp.float32).astype(jnp.bfloat16)
    value_up = jnp.dot(normed, value_full, preferred_element_type=jnp.float32).astype(jnp.bfloat16)
    hidden_width = gate_up.shape[1]
    stacked = jnp.concatenate([gate_up, value_up], axis=1)
    edged_up = extended(stacked, (("sp", 0),), 1).astype(jnp.float32)
    taps = jnp.concatenate([conv_gate, conv_value], axis=1).astype(jnp.float32)
    convolved = edged_up[:-2] * taps[0] + edged_up[1:-1] * taps[1] + edged_up[2:] * taps[2]
    hidden = (jax.nn.silu(convolved[:, :hidden_width]) * convolved[:, hidden_width:]).astype(
        jnp.bfloat16
    )
    terms = jnp.dot(
        hidden, lax.all_gather(w_down, "sp", axis=1, tiled=True), preferred_element_type=jnp.float32
    )
    ffn_rows = lax.psum_scatter(
        terms.astype(jnp.bfloat16), "tp", scatter_dimension=0, tiled=True
    ).astype(jnp.float32)
    return (mid_rows.astype(jnp.float32) + ffn_rows).astype(jnp.bfloat16)


F32 = jnp.float32
BF16 = jnp.bfloat16
PAIR = 2
EDGE = 8


def layer_kernel(
    sp,
    tp,
    q_ref,
    band_ref,
    cos_ref,
    sin_ref,
    base_ref,
    sink_ref,
    res_ref,
    gain_ref,
    wo_ref,
    wg_ref,
    wv_ref,
    tg_ref,
    tv_ref,
    wd_ref,
    out_ref,
    band,
    key_value,
    value_key,
    att,
    att_all,
    wo,
    wg,
    wv,
    wd,
    mid,
    normed,
    upg,
    upv,
    hidden,
    terms,
    near,
    pair_sum,
    first_x,
    first_y,
    sum_x,
    sum_y,
    last_x,
    last_y,
    tapg,
    tapv,
    local_sem,
    w_send,
    w_recv,
    wo_send,
    wo_recv,
    att_send,
    att_recv,
    kv_send,
    kv_recv,
    edge_send,
    edge_recv,
    n_send,
    n_recv,
    r_send,
    r_recv,
):
    me = lax.axis_index("sp")
    my_tp = lax.axis_index("tp")
    tok = q_ref.shape[0]
    share, width = mid.shape
    group = normed.shape[0]
    line = sp // PAIR
    place = me // PAIR
    side = me % PAIR
    mate = place * PAIR + (1 - side)
    depth = wg_ref.shape[0]
    wide = wg.shape[1]
    cols = wd_ref.shape[1]
    lane_half = cols // 2
    has_low = me > 0
    has_high = me < sp - 1
    can_down = place > 0
    can_up = place < line - 1
    end_down = place == 1
    end_up = place == line - 2
    row_y = my_tp // 2
    core = my_tp % 2
    buddy = my_tp + 1 - 2 * core
    across = lax.rem(my_tp + 2, tp)
    corner = lax.rem(buddy + 2, tp)

    def remote(src, dst, send, recv, **where):
        return pltpu.make_async_remote_copy(
            src_ref=src,
            dst_ref=dst,
            send_sem=send,
            recv_sem=recv,
            device_id=where,
            device_id_type=pl.DeviceIdType.MESH,
        )

    barrier = pltpu.get_barrier_semaphore()

    def greet(**where):
        pl.semaphore_signal(
            barrier, inc=1, device_id=where, device_id_type=pl.DeviceIdType.MESH
        )

    greet(sp=mate)
    for peer in (buddy, across, corner):
        greet(tp=peer)
    far_low = has_low & (side == 0)
    far_high = has_high & (side == PAIR - 1)
    pl.when(far_low)(lambda: greet(sp=me - 1))
    pl.when(far_high)(lambda: greet(sp=me + 1))
    pl.when(can_down)(lambda: greet(sp=me - PAIR))
    pl.when(can_up)(lambda: greet(sp=me + PAIR))
    count = tp
    for able in (far_low, far_high, can_down, can_up):
        count = count + jnp.where(able, 1, 0)
    pl.semaphore_wait(barrier, count)

    def w_part(kind, half):
        start = pl.multiple_of(half * wide, wide)
        if kind == 2:
            return wd_ref.at[pl.ds(start, wide), :]
        return (wg_ref, wv_ref)[kind].at[:, pl.ds(start, wide)]

    def w_slot(kind, block):
        if kind == 2:
            return wd.at[block]
        return (wg, wv)[kind].at[pl.ds(pl.multiple_of(block * depth, depth), depth), :]

    def w_copy(kind, block, way, own=False):
        slot = w_slot(kind, block)
        src = w_part(kind, 1 - side if way == 2 else side) if own else slot
        return remote(
            src,
            slot,
            w_send.at[kind, block, way],
            w_recv.at[kind, block],
            sp=(me - PAIR, me + PAIR, mate)[way],
        )

    def step(s):
        reach = jnp.minimum(place, line - 1 - place)
        far = (s + 1) // 2
        swing = jnp.where(s % 2 == 1, place + far, place - far)
        rest = jnp.where(2 * place < line - 1, s, line - 1 - s)
        there = jnp.where(s <= 2 * reach, swing, rest)
        return there, there > place

    def forwards(above):
        return (above & can_down) | (jnp.logical_not(above) & can_up)

    def block_of(there, other):
        return there * PAIR + (1 - side if other else side)

    def relay(s, kind, other):
        there, above = step(s)
        block = block_of(there, other)

        @pl.when(forwards(above))
        def _():
            w_copy(kind, block, 2).wait_recv()
            pl.when(above & can_down)(w_copy(kind, block, 0).start)
            pl.when(jnp.logical_not(above) & can_up)(w_copy(kind, block, 1).start)

    def settle(s, kind, other):
        there, above = step(s)
        block = block_of(there, other)
        pl.when(jnp.logical_not(forwards(above)))(w_copy(kind, block, 2).wait_recv)

    kv_low = remote(
        band_ref.at[pl.ds(0, WINDOW), :],
        band.at[pl.ds(WINDOW + tok, WINDOW), :],
        kv_send.at[0],
        kv_recv.at[1],
        sp=me - 1,
    )
    kv_high = remote(
        band_ref.at[pl.ds(tok - WINDOW, WINDOW), :],
        band.at[pl.ds(0, WINDOW), :],
        kv_send.at[1],
        kv_recv.at[0],
        sp=me + 1,
    )

    def shares(index, half=None):
        if half is None:
            return pl.ds(pl.multiple_of(index * share, share), share)
        size = share // 2
        return pl.ds(pl.multiple_of(index * share + half * size, size), size)

    own_local = [
        pltpu.make_async_copy(band_ref, band.at[pl.ds(WINDOW, tok), :], local_sem.at[0]),
        pltpu.make_async_copy(wo_ref, wo.at[my_tp], local_sem.at[1]),
        pltpu.make_async_copy(res_ref.at[shares(my_tp), :], mid, local_sem.at[2]),
    ] + [
        pltpu.make_async_copy(w_part(kind, side), w_slot(kind, me), local_sem.at[3 + kind])
        for kind in range(3)
    ]

    def wo_copy(k, own=True):
        slot = wo.at[my_tp if own else across]
        return remote(
            wo_ref if own else slot,
            slot,
            wo_send.at[k],
            wo_recv.at[my_tp if own else across],
            tp=(buddy, across, buddy)[k],
        )

    def arrived(ref, recv, source):
        slot = ref.at[source]
        return remote(slot, slot, wo_send.at[0], recv.at[source], tp=buddy)

    pl.when(has_low)(kv_low.start)
    pl.when(has_high)(kv_high.start)
    for copy in own_local:
        copy.start()
    for kind in range(2):
        w_copy(kind, me, 2, True).start()
        pl.when(can_down)(w_copy(kind, me, 0, True).start)
        pl.when(can_up)(w_copy(kind, me, 1, True).start)
    w_copy(2, me, 2, True).start()
    wo_copy(1).start()
    wo_copy(0).start()

    for ref, taps in ((tg_ref, tapg), (tv_ref, tapv)):
        taps[...] = jnp.where(side == 0, ref[:, 0:wide], ref[:, wide : 2 * wide]).astype(F32)

    blank = jnp.zeros((WINDOW, band.shape[1]), BF16)

    @pl.when(jnp.logical_not(has_low))
    def _():
        band[pl.ds(0, WINDOW), :] = blank

    @pl.when(jnp.logical_not(has_high))
    def _():
        band[pl.ds(WINDOW + tok, WINDOW), :] = blank

    own_local[0].wait()
    pl.when(has_low)(kv_high.wait_recv)
    pl.when(has_high)(kv_low.wait_recv)
    heads = q_ref.shape[1] // HD
    span = 3 * WINDOW
    total = tok * sp
    lane = lax.broadcasted_iota(jnp.int32, (WINDOW, 2 * HD), 1)
    early = lane % HD < HD // 2
    low = lane < HD

    def turn(field, start):
        rows = pl.ds(start, WINDOW)
        base_cos = base_ref[0:1, :]
        base_sin = base_ref[1:2, :]
        cosine = base_cos * cos_ref[rows, :] - base_sin * sin_ref[rows, :]
        sine = base_sin * cos_ref[rows, :] + base_cos * sin_ref[rows, :]
        ahead = pltpu.roll(field, 2 * HD - HD // 2, 1)
        behind = pltpu.roll(field, HD // 2, 1)
        return field * cosine + jnp.where(early, -ahead, behind) * sine

    def turn_keys(i, carry):
        start = pl.multiple_of(i * WINDOW, WINDOW)
        field = band[pl.ds(start, WINDOW), :].astype(F32)
        field = jnp.where(low, turn(field, start), field)
        key_value[pl.ds(start, WINDOW), :] = field.astype(BF16)
        value_key[pl.ds(start, WINDOW), :] = pltpu.roll(field, HD, 1).astype(BF16)
        return carry

    lax.fori_loop(0, tok // WINDOW + 2, turn_keys, 0)

    def att_copy(k):
        peer = (corner, across, buddy)[k]
        return remote(
            att.at[shares(peer), :],
            att_all.at[my_tp],
            att_send.at[k],
            att_recv.at[my_tp],
            tp=peer,
        )

    per = share // WINDOW

    def attend(i, carry):
        k = i // per
        target = jnp.where(
            k == 0, corner, jnp.where(k == 1, across, jnp.where(k == 2, buddy, my_tp))
        )
        start = pl.multiple_of(target * share + i % per * WINDOW, WINDOW)
        straight = key_value[pl.ds(start, span), :]
        crossed = value_key[pl.ds(start, span), :]
        row = lax.broadcasted_iota(jnp.int32, (WINDOW, span), 0)
        col = lax.broadcasted_iota(jnp.int32, (WINDOW, span), 1)
        key_pos = col + (me * tok - WINDOW + start)
        valid = (col >= row) & (col <= row + 2 * WINDOW) & (key_pos >= 0) & (key_pos < total)

        def head(query, sink, keys, values):
            scores = lax.dot_general(
                query, keys, (((1,), (1,)), ((), ())), preferred_element_type=F32
            )
            scores = jnp.where(valid, scores, -1e30)
            top = jnp.maximum(jnp.max(scores, axis=-1, keepdims=True), sink)
            weights = jnp.exp(scores - top)
            denom = jnp.sum(weights, axis=-1, keepdims=True) + jnp.exp(sink - top)
            probs = (weights * (1.0 / denom)).astype(BF16)
            return jnp.dot(probs, values, preferred_element_type=F32)

        for h in range(0, heads, 2):
            lanes = pl.ds(h * HD, 2 * HD)
            field = q_ref[pl.ds(start, WINDOW), lanes].astype(F32)
            field = turn(field, pl.multiple_of(start + WINDOW, WINDOW)) * HD**-0.5
            even = head(
                jnp.where(low, field, 0.0).astype(BF16), sink_ref[h], straight, crossed
            )
            odd = head(
                jnp.where(low, 0.0, field).astype(BF16), sink_ref[h + 1], crossed, straight
            )
            att[pl.ds(start, WINDOW), lanes] = jnp.where(low, even, odd).astype(BF16)
        for n in range(tp - 1):
            pl.when(i == per * (n + 1) - 1)(att_copy(n).start)

        @pl.when(i == per * 2 - 1)
        def _():
            for kind in range(2):
                w_copy(kind, mate, 2).wait_recv()
                pl.when(can_down)(w_copy(kind, mate, 0).start)
                pl.when(can_up)(w_copy(kind, mate, 1).start)
            for kind in range(2):
                for s in (1, 2):
                    if s < line:
                        relay(s, kind, False)

        return carry

    lax.fori_loop(0, tok // WINDOW, attend, 0)
    att_all[my_tp] = att[shares(my_tp), :]
    for kind in range(2):
        for s in (1, 2):
            if s < line:
                relay(s, kind, True)
    arrived(wo, wo_recv, across).wait_recv()
    wo_copy(2, False).start()

    own_local[1].wait()
    own_local[2].wait()
    for source in (buddy, across, corner):
        if source is not across:
            arrived(wo, wo_recv, source).wait_recv()
        arrived(att_all, att_recv, source).wait_recv()
    piece = 512
    mine = side * tp + my_tp
    squares = jnp.zeros((share, 1), F32)
    for c in range(0, width, piece):
        acc = jnp.zeros((share, piece), F32)
        for k in range(tp):
            term = jnp.dot(att_all[k], wo[k, :, pl.ds(c, piece)], preferred_element_type=F32)
            acc = acc + term.astype(BF16).astype(F32)
        new = (mid[:, pl.ds(c, piece)].astype(F32) + acc).astype(BF16)
        mid[:, pl.ds(c, piece)] = new
        field = new.astype(F32)
        squares = squares + jnp.sum(field * field, axis=-1, keepdims=True)
    scale = lax.rsqrt(squares * (1.0 / width) + EPS)
    for c in range(0, width, piece):
        field = mid[:, pl.ds(c, piece)].astype(F32)
        normed[shares(mine), pl.ds(c, piece)] = (
            field * scale * gain_ref[:, pl.ds(c, piece)]
        ).astype(BF16)

    from_mate = (1 - side) * tp + my_tp
    from_across = side * tp + across
    from_corner = side * tp + corner
    diagonal = (1 - side) * tp + across
    rows_sent = [
        (mine, None, "buddy"),
        (mine, None, "mate"),
        (mine, None, "across"),
        (from_mate, None, "buddy"),
        (from_mate, 0, "across"),
        (from_across, None, "buddy"),
        (from_across, 1, "mate"),
        (diagonal, 0, "buddy"),
        (diagonal, 1, "buddy"),
    ]

    def n_copy(k):
        index, half, goal = rows_sent[k]
        slot = normed.at[shares(index, half), :]
        where = {"sp": mate} if goal == "mate" else {"tp": buddy if goal == "buddy" else across}
        return remote(slot, slot, n_send.at[k], n_recv.at[index, half or 0], **where)

    def n_wait(index, half=None):
        slot = normed.at[shares(index, half), :]
        remote(slot, slot, n_send.at[0], n_recv.at[index, half or 0], tp=buddy).wait_recv()

    for k in (1, 2, 0):
        n_copy(k).start()

    def relay_all(steps, kinds, other):
        for s in steps:
            if s < line:
                for kind in kinds:
                    relay(s, kind, other)

    relay_all(range(3, line), (0, 1), False)
    relay_all(range(3, line), (0, 1), True)

    w_copy(2, mate, 2).wait_recv()

    def start_down(down, up):
        pl.when(down)(w_copy(2, me, 0, True).start)
        pl.when(up)(w_copy(2, me, 1, True).start)
        pl.when(down)(w_copy(2, mate, 0).start)
        pl.when(up)(w_copy(2, mate, 1).start)

    start_down(can_down & jnp.logical_not(end_down), can_up & jnp.logical_not(end_up))
    n_wait(from_mate)
    n_copy(4).start()
    n_copy(3).start()
    n_wait(from_across)
    n_copy(6).start()
    n_copy(5).start()
    for s in range(1, line):
        for other in (False, True):
            for kind in range(2):
                settle(s, kind, other)
    for kind in range(2):
        own_local[3 + kind].wait()
    for half in range(2):
        n_wait(diagonal, half)
        n_copy(7 + half).start()
    n_wait(side * tp + buddy)
    n_wait(from_corner)
    n_wait((1 - side) * tp + buddy)
    for half in range(2):
        n_wait((1 - side) * tp + corner, half)

    tile = share
    tiles = group // tile

    def project(i):
        base = pl.multiple_of(i * tile, tile)
        left = normed[pl.ds(base, tile), :]
        rows = pl.ds(pl.multiple_of(base + EDGE, EDGE), tile)
        for weight, dest in ((wg, upg), (wv, upv)):
            term = jnp.dot(left, weight[...], preferred_element_type=F32)
            dest[rows, :] = term.astype(BF16).astype(F32)

    def project_step(i, carry):
        project(i)
        return carry

    def edge_low(kind):
        ref = (upg, upv)[kind]
        return remote(
            ref.at[pl.ds(EDGE, EDGE), :],
            ref.at[pl.ds(EDGE + group, EDGE), :],
            edge_send.at[0, kind],
            edge_recv.at[1, kind],
            sp=me - PAIR,
        )

    def edge_high(kind):
        ref = (upg, upv)[kind]
        return remote(
            ref.at[pl.ds(group, EDGE), :],
            ref.at[pl.ds(0, EDGE), :],
            edge_send.at[1, kind],
            edge_recv.at[0, kind],
            sp=me + PAIR,
        )

    def project_edge(i, carry):
        project(i * (tiles - 1))
        return carry

    lax.fori_loop(0, 2, project_edge, 0)
    for kind in range(2):
        pl.when(can_down)(edge_low(kind).start)
        pl.when(can_up)(edge_high(kind).start)
    start_down(can_down & end_down, can_up & end_up)
    relay_all((1, 2), (2,), False)
    relay_all((1, 2), (2,), True)
    lax.fori_loop(1, tiles - 1, project_step, 0)

    none = jnp.zeros((EDGE, wide), F32)

    @pl.when(jnp.logical_not(can_down))
    def _():
        upg[pl.ds(0, EDGE), :] = none
        upv[pl.ds(0, EDGE), :] = none

    @pl.when(jnp.logical_not(can_up))
    def _():
        upg[pl.ds(EDGE + group, EDGE), :] = none
        upv[pl.ds(EDGE + group, EDGE), :] = none

    for kind in range(2):
        pl.when(can_down)(edge_high(kind).wait_recv)
        pl.when(can_up)(edge_low(kind).wait_recv)

    def gate(i, carry):
        base = pl.multiple_of(i * WINDOW, WINDOW)
        for c in range(0, wide, 256):
            lanes = pl.ds(c, 256)

            def convolve(ref, taps):
                field = ref[pl.ds(base, WINDOW + 2 * EDGE), lanes]
                return (
                    field[EDGE - 1 : EDGE - 1 + WINDOW] * taps[0:1, lanes]
                    + field[EDGE : EDGE + WINDOW] * taps[1:2, lanes]
                    + field[EDGE + 1 : EDGE + 1 + WINDOW] * taps[2:3, lanes]
                )

            g = convolve(upg, tapg)
            v = convolve(upv, tapv)
            hidden[pl.ds(base, WINDOW), lanes] = (g / (1.0 + jnp.exp(-g)) * v).astype(BF16)
        return carry

    lax.fori_loop(0, group // WINDOW, gate, 0)
    relay_all(range(3, line), (2,), False)

    front = pl.ds(0, lane_half)
    back = pl.ds(lane_half, lane_half)

    def r_copy(k, block):
        src, dst = (
            (terms.at[block, :, :, 1 - core], near.at[block]),
            (pair_sum.at[block, 1 - side, :, :, front], first_x.at[block]),
            (pair_sum.at[block, :, 1 - row_y, :, back], first_y.at[block]),
            (sum_x.at[block], last_x.at[block]),
            (sum_y.at[block], last_y.at[block]),
        )[k]
        where = ({"tp": buddy}, {"sp": mate}, {"tp": across}, {"tp": across}, {"sp": mate})[k]
        return remote(src, dst, r_send.at[k, block], r_recv.at[k, block], **where)

    def block_at(j):
        there, _ = step(j // 2)
        return there * PAIR + jnp.where(j % 2 == 0, side, 1 - side)

    def produce(j):
        block = block_at(j)

        @pl.when(j == 0)
        def _():
            own_local[5].wait()

        @pl.when(j == 2)
        def _():
            relay_all(range(3, line), (2,), True)

        @pl.when(j > 1)
        def _():
            there, above = step(j // 2)
            pl.when(jnp.logical_not(forwards(above)))(w_copy(2, block, 2).wait_recv)

        def part(i, carry):
            rows = pl.ds(pl.multiple_of(i * 2 * share, 2 * share), 2 * share)
            term = jnp.dot(hidden[rows, :], wd[block], preferred_element_type=F32)
            terms[block, i // 2, i % 2] = term.astype(BF16).reshape(2, share, cols)
            return carry

        lax.fori_loop(0, group // (2 * share), part, 0)
        r_copy(0, block).start()

    def pass_first(j):
        block = block_at(j)
        r_copy(0, block).wait_recv()
        for x in range(PAIR):
            for y in range(tp // 2):
                both = terms[block, x, y, core].astype(F32) + near[block, x, y].astype(F32)
                pair_sum[block, x, y] = both.astype(BF16)
        r_copy(1, block).start()
        r_copy(2, block).start()

    def pass_second(j):
        block = block_at(j)
        r_copy(1, block).wait_recv()
        both = pair_sum[block, side, 1 - row_y, :, front].astype(F32)
        sum_x[block] = (both + first_x[block, 1 - row_y].astype(F32)).astype(BF16)
        r_copy(3, block).start()
        r_copy(2, block).wait_recv()
        both = pair_sum[block, 1 - side, row_y, :, back].astype(F32)
        sum_y[block] = (both + first_y[block, 1 - side].astype(F32)).astype(BF16)
        r_copy(4, block).start()

    def down(j, carry):
        pl.when(j < sp)(lambda: produce(j))
        pl.when((j > 0) & (j < sp + 1))(lambda: pass_first(j - 1))
        pl.when(j > 1)(lambda: pass_second(j - 2))
        return carry

    lax.fori_loop(0, sp + 2, down, 0)

    for block in range(sp):
        r_copy(3, block).wait_recv()
        r_copy(4, block).wait_recv()
        for half in range(2):
            part = (front, back)[half]
            first = first_x[block, row_y] if half == 0 else first_y[block, side]
            last = last_x[block] if half == 0 else last_y[block]
            lanes = pl.ds(block * cols + half * lane_half, lane_half)
            acc = mid[:, lanes].astype(F32) + pair_sum[block, side, row_y, :, part].astype(F32)
            acc = acc + first.astype(F32) + last.astype(F32)
            out_ref[:, lanes] = acc.astype(BF16)

    for kind in range(3):
        w_copy(kind, me, 2, True).wait_send()
        for block in (me, mate):
            pl.when(can_down)(w_copy(kind, block, 0).wait_send)
            pl.when(can_up)(w_copy(kind, block, 1).wait_send)

    def drain(s, carry):
        there, above = step(s)
        for kind in range(3):
            for other in (False, True):
                block = block_of(there, other)
                pl.when(above & can_down)(w_copy(kind, block, 0).wait_send)
                pl.when(jnp.logical_not(above) & can_up)(w_copy(kind, block, 1).wait_send)
        return carry

    lax.fori_loop(1, line, drain, 0)
    for k in range(tp - 1):
        wo_copy(k, k < 2).wait_send()
        att_copy(k).wait_send()
    for k in range(len(rows_sent)):
        n_copy(k).wait_send()
    pl.when(has_low)(kv_low.wait_send)
    pl.when(has_high)(kv_high.wait_send)
    for kind in range(2):
        pl.when(can_down)(edge_low(kind).wait_send)
        pl.when(can_up)(edge_high(kind).wait_send)

    def drain_sums(block, carry):
        for k in range(5):
            r_copy(k, block).wait_send()
        return carry

    lax.fori_loop(0, sp, drain_sums, 0)


def kernel_shards(
    sp,
    tp,
    residual,
    query,
    key,
    value,
    sink,
    norm_gain,
    w_out,
    w_gate,
    w_value,
    conv_gate,
    conv_value,
    w_down,
):
    tok, width = residual.shape
    depth, hid = w_gate.shape
    cols = w_down.shape[1]
    heads = query.shape[1] // HD
    share = tok // tp
    wide = hid // PAIR
    group = PAIR * tok
    offset = lax.axis_index("sp") * tok
    band = jnp.concatenate([key, value], axis=1)
    inverse = THETA ** (-(np.arange(2 * HD) % (HD // 2)) * 2.0 / HD)
    angle = (np.arange(tok + 2 * WINDOW) - WINDOW)[:, None] * inverse[None, :]
    first = offset.astype(F32) * jnp.asarray(inverse, F32)
    base = jnp.stack([jnp.cos(first), jnp.sin(first)])
    vmem = pl.BlockSpec(memory_space=pltpu.VMEM)
    smem = pl.BlockSpec(memory_space=pltpu.SMEM)
    anywhere = pl.BlockSpec(memory_space=pl.ANY)
    dma = pltpu.SemaphoreType.DMA
    return pl.pallas_call(
        functools.partial(layer_kernel, sp, tp),
        out_shape=jax.ShapeDtypeStruct((tok // tp, width), BF16),
        in_specs=[vmem] * 5 + [smem, anywhere, vmem] + [anywhere] * 3 + [vmem] * 2 + [anywhere],
        out_specs=vmem,
        scratch_shapes=[
            pltpu.VMEM((tok + 2 * WINDOW, 2 * HD), BF16),
            pltpu.VMEM((tok + 2 * WINDOW, 2 * HD), BF16),
            pltpu.VMEM((tok + 2 * WINDOW, 2 * HD), BF16),
            pltpu.VMEM((tok, heads * HD), BF16),
            pltpu.VMEM((tp, share, heads * HD), BF16),
            pltpu.VMEM((tp,) + w_out.shape, BF16),
            pltpu.VMEM((sp * depth, wide), BF16),
            pltpu.VMEM((sp * depth, wide), BF16),
            pltpu.VMEM((sp, wide, cols), BF16),
            pltpu.VMEM((share, width), BF16),
            pltpu.VMEM((group, width), BF16),
            pltpu.VMEM((group + 2 * EDGE, wide), F32),
            pltpu.VMEM((group + 2 * EDGE, wide), F32),
            pltpu.VMEM((group, wide), BF16),
            pltpu.VMEM((sp, PAIR, tp // 2, 2, share, cols), BF16),
            pltpu.VMEM((sp, PAIR, tp // 2, share, cols), BF16),
            pltpu.VMEM((sp, PAIR, tp // 2, share, cols), BF16),
            pltpu.VMEM((sp, tp // 2, share, cols // 2), BF16),
            pltpu.VMEM((sp, PAIR, share, cols // 2), BF16),
            pltpu.VMEM((sp, share, cols // 2), BF16),
            pltpu.VMEM((sp, share, cols // 2), BF16),
            pltpu.VMEM((sp, share, cols // 2), BF16),
            pltpu.VMEM((sp, share, cols // 2), BF16),
            pltpu.VMEM((3, wide), F32),
            pltpu.VMEM((3, wide), F32),
            dma((6,)),
            dma((3, sp, 3)),
            dma((3, sp)),
            dma((tp - 1,)),
            dma((tp,)),
            dma((tp - 1,)),
            dma((tp,)),
            dma((2,)),
            dma((2,)),
            dma((2, 2)),
            dma((2, 2)),
            dma((9,)),
            dma((PAIR * tp, 2)),
            dma((5, sp)),
            dma((5, sp)),
        ],
        compiler_params=pltpu.CompilerParams(
            collective_id=0, has_side_effects=True, vmem_limit_bytes=66 * 1000 * 1000
        ),
        name="layer",
    )(
        query,
        band,
        jnp.asarray(np.cos(angle), F32),
        jnp.asarray(np.sin(angle), F32),
        base,
        sink,
        residual,
        norm_gain.reshape(1, -1),
        w_out,
        w_gate,
        w_value,
        conv_gate,
        conv_value,
        w_down,
    )


def solution(mesh):
    sp, tp = mesh.shape["sp"], mesh.shape["tp"]

    def shards(*args):
        if args[11].shape[1] % 256 or sp % PAIR or tp != 4 or args[2].shape[1] != HD:
            return plain_shards(*args)
        return kernel_shards(sp, tp, *args)

    return jax.shard_map(
        shards,
        mesh=mesh,
        in_specs=(
            P("sp", None),
            P("sp", "tp"),
            P("sp", "tp"),
            P("sp", "tp"),
            P("tp"),
            P(),
            P("tp", None),
            P("sp", "tp"),
            P("sp", "tp"),
            P(None, "tp"),
            P(None, "tp"),
            P("tp", "sp"),
        ),
        out_specs=P(("sp", "tp"), None),
        check_vma=False,
    )
```

```python
import functools

import jax
import jax.numpy as jnp
import numpy as np
from jax import lax
from jax.experimental import pallas as pl
from jax.experimental.pallas import tpu as pltpu
from jax.sharding import PartitionSpec as P

HD = 64
WINDOW = 128


THETA = 10000.0
EPS = 1e-06


def extended(block, sides, width):
    for axis, dim in sides:
        count = lax.axis_size(axis)
        forward = [(i, i + 1) for i in range(count - 1)]
        backward = [(target, source) for source, target in forward]
        low = lax.ppermute(
            lax.slice_in_dim(block, block.shape[dim] - width, None, axis=dim), axis, forward
        )
        high = lax.ppermute(lax.slice_in_dim(block, 0, width, axis=dim), axis, backward)
        block = jnp.concatenate([low, block, high], axis=dim)
    return block


def rotate(field, positions):
    count = field.shape[0]
    parts = field.astype(jnp.float32).reshape(count, -1, HD)
    inverse = 1.0 / THETA ** (jnp.arange(0, HD, 2, dtype=jnp.float32) / HD)
    angle = positions[:, None] * inverse[None, :]
    cosine = jnp.cos(angle)[:, None, :]
    sine = jnp.sin(angle)[:, None, :]
    first = parts[..., : HD // 2]
    second = parts[..., HD // 2 :]
    turned = jnp.concatenate(
        [first * cosine - second * sine, second * cosine + first * sine], axis=-1
    )
    return turned.reshape(count, -1).astype(jnp.bfloat16)


def band_attention(queries, keys, values, sinks, start, total):
    count = queries.shape[0]
    blocks = count // WINDOW
    kv_local = keys.shape[1] // HD
    group = queries.shape[1] // (kv_local * HD)
    query_blocks = queries.reshape(blocks, WINDOW, kv_local, group, HD)
    key_band = jnp.concatenate(
        [
            keys[i * WINDOW : i * WINDOW + count].reshape(blocks, WINDOW, kv_local, HD)
            for i in range(3)
        ],
        axis=1,
    )
    value_band = jnp.concatenate(
        [
            values[i * WINDOW : i * WINDOW + count].reshape(blocks, WINDOW, kv_local, HD)
            for i in range(3)
        ],
        axis=1,
    )
    scores = jnp.einsum(
        "nqkgd,njkd->nkgqj", query_blocks, key_band, preferred_element_type=jnp.float32
    ) * HD ** (-0.5)
    block_ids = jnp.arange(blocks, dtype=jnp.int32)[:, None]
    query_pos = start + block_ids * WINDOW + jnp.arange(WINDOW, dtype=jnp.int32)[None, :]
    key_pos = start - WINDOW + block_ids * WINDOW + jnp.arange(3 * WINDOW, dtype=jnp.int32)[None, :]
    valid = (
        (key_pos[:, None, :] >= 0)
        & (key_pos[:, None, :] < total)
        & (jnp.abs(query_pos[:, :, None] - key_pos[:, None, :]) <= WINDOW)
    )
    scores = jnp.where(valid[:, None, None], scores, -1e30)
    sink_col = sinks.reshape(1, kv_local, group, 1, 1)
    top = jnp.maximum(jnp.max(scores, axis=-1, keepdims=True), sink_col)
    weights = jnp.exp(scores - top)
    denom = jnp.sum(weights, axis=-1, keepdims=True) + jnp.exp(sink_col - top)
    probs = (weights / denom).astype(jnp.bfloat16)
    out = jnp.einsum("nkgqj,njkd->nqkgd", probs, value_band, preferred_element_type=jnp.float32)
    return out.reshape(count, kv_local * group * HD).astype(jnp.bfloat16)


def rmsnorm(field, gain):
    wide = field.astype(jnp.float32)
    scale = lax.rsqrt(jnp.mean(wide * wide, axis=-1, keepdims=True) + EPS)
    return (wide * scale * gain).astype(jnp.bfloat16)


def plain_shards(
    residual,
    query,
    key,
    value,
    sink,
    norm_gain,
    w_out,
    w_gate,
    w_value,
    conv_gate,
    conv_value,
    w_down,
):
    tok_rows = query.shape[0]
    offset = lax.axis_index("sp") * tok_rows
    total = tok_rows * lax.axis_size("sp")
    share = tok_rows // lax.axis_size("tp")
    tp_index = lax.axis_index("tp")
    positions = (offset + jnp.arange(tok_rows, dtype=jnp.int32)).astype(jnp.float32)
    turned_query = rotate(query, positions)
    turned_key = rotate(key, positions)
    key_width = key.shape[1]
    band = jnp.concatenate([turned_key, value], axis=1)
    edged = extended(band, (("sp", 0),), WINDOW)
    attended = band_attention(
        turned_query, edged[:, :key_width], edged[:, key_width:], sink, offset, total
    )
    partial_value = jnp.dot(attended, w_out, preferred_element_type=jnp.float32)
    mix_full = lax.psum(partial_value.astype(jnp.bfloat16), "tp").astype(jnp.float32)
    mid_full = (residual.astype(jnp.float32) + mix_full).astype(jnp.bfloat16)
    normed = rmsnorm(mid_full, norm_gain)
    mid_rows = lax.dynamic_slice_in_dim(mid_full, tp_index * share, share, 0)
    gate_full, value_full = (
        lax.all_gather(w_gate, "sp", axis=0, tiled=True),
        lax.all_gather(w_value, "sp", axis=0, tiled=True),
    )
    gate_up = jnp.dot(normed, gate_full, preferred_element_type=jnp.float32).astype(jnp.bfloat16)
    value_up = jnp.dot(normed, value_full, preferred_element_type=jnp.float32).astype(jnp.bfloat16)
    hidden_width = gate_up.shape[1]
    stacked = jnp.concatenate([gate_up, value_up], axis=1)
    edged_up = extended(stacked, (("sp", 0),), 1).astype(jnp.float32)
    taps = jnp.concatenate([conv_gate, conv_value], axis=1).astype(jnp.float32)
    convolved = edged_up[:-2] * taps[0] + edged_up[1:-1] * taps[1] + edged_up[2:] * taps[2]
    hidden = (jax.nn.silu(convolved[:, :hidden_width]) * convolved[:, hidden_width:]).astype(
        jnp.bfloat16
    )
    terms = jnp.dot(
        hidden, lax.all_gather(w_down, "sp", axis=1, tiled=True), preferred_element_type=jnp.float32
    )
    ffn_rows = lax.psum_scatter(
        terms.astype(jnp.bfloat16), "tp", scatter_dimension=0, tiled=True
    ).astype(jnp.float32)
    return (mid_rows.astype(jnp.float32) + ffn_rows).astype(jnp.bfloat16)


F32 = jnp.float32
BF16 = jnp.bfloat16
PAIR = 2
EDGE = 8


def layer_kernel(
    sp,
    tp,
    q_ref,
    k_ref,
    v_ref,
    table_ref,
    sink_ref,
    res_ref,
    gain_ref,
    wo_ref,
    wg_ref,
    wv_ref,
    tg_ref,
    tv_ref,
    wd_ref,
    out_ref,
    q,
    table,
    band,
    key_value,
    value_key,
    att,
    att_all,
    wo,
    wg,
    wv,
    wd,
    mid,
    normed,
    upg,
    upv,
    hidden,
    terms,
    near,
    pair_sum,
    first_x,
    first_y,
    sum_x,
    sum_y,
    last_x,
    last_y,
    tapg,
    tapv,
    local_sem,
    w_send,
    w_recv,
    wo_send,
    wo_recv,
    att_send,
    att_recv,
    kv_send,
    kv_recv,
    edge_send,
    edge_recv,
    n_send,
    n_recv,
    r_send,
    r_recv,
):
    me = lax.axis_index("sp")
    my_tp = lax.axis_index("tp")
    tok = q.shape[0]
    share, width = mid.shape
    group = normed.shape[0]
    line = sp // PAIR
    place = me // PAIR
    side = me % PAIR
    mate = place * PAIR + (1 - side)
    depth = wg_ref.shape[0]
    wide = wg.shape[1]
    cols = wd_ref.shape[1]
    lane_half = cols // 2
    has_low = me > 0
    has_high = me < sp - 1
    can_down = place > 0
    can_up = place < line - 1
    end_down = place == 1
    end_up = place == line - 2
    row_y = my_tp // 2
    core = my_tp % 2
    buddy = my_tp + 1 - 2 * core
    across = lax.rem(my_tp + 2, tp)
    corner = lax.rem(buddy + 2, tp)

    def remote(src, dst, send, recv, **where):
        return pltpu.make_async_remote_copy(
            src_ref=src,
            dst_ref=dst,
            send_sem=send,
            recv_sem=recv,
            device_id=where,
            device_id_type=pl.DeviceIdType.MESH,
        )

    barrier = pltpu.get_barrier_semaphore()

    def greet(**where):
        pl.semaphore_signal(
            barrier, inc=1, device_id=where, device_id_type=pl.DeviceIdType.MESH
        )

    def own_band(i):
        lanes = pl.ds(i * WINDOW, WINDOW)
        pair = jnp.concatenate([k_ref[:, lanes], v_ref[:, lanes]], axis=0)
        band[pl.ds((i + 1) * WINDOW, WINDOW), :] = pair.astype(F32).T.astype(BF16)

    greet(sp=mate)
    for peer in (buddy, across, corner):
        greet(tp=peer)
    far_low = has_low & (side == 0)
    far_high = has_high & (side == PAIR - 1)
    pl.when(far_low)(lambda: greet(sp=me - 1))
    pl.when(far_high)(lambda: greet(sp=me + 1))
    pl.when(can_down)(lambda: greet(sp=me - PAIR))
    pl.when(can_up)(lambda: greet(sp=me + PAIR))
    count = tp
    for able in (far_low, far_high, can_down, can_up):
        count = count + jnp.where(able, 1, 0)
    early_local = [
        pltpu.make_async_copy(q_ref, q, local_sem.at[0]),
        pltpu.make_async_copy(table_ref, table, local_sem.at[6]),
    ]
    for copy in early_local:
        copy.start()
    own_band(0)
    own_band(tok // WINDOW - 1)
    pl.semaphore_wait(barrier, count)

    def w_part(kind, half):
        start = pl.multiple_of(half * wide, wide)
        if kind == 2:
            return wd_ref.at[pl.ds(start, wide), :]
        return (wg_ref, wv_ref)[kind].at[:, pl.ds(start, wide)]

    def w_slot(kind, block):
        if kind == 2:
            return wd.at[block]
        return (wg, wv)[kind].at[pl.ds(pl.multiple_of(block * depth, depth), depth), :]

    def w_copy(kind, block, way, own=False):
        slot = w_slot(kind, block)
        src = w_part(kind, 1 - side if way == 2 else side) if own else slot
        return remote(
            src,
            slot,
            w_send.at[kind, block, way],
            w_recv.at[kind, block],
            sp=(me - PAIR, me + PAIR, mate)[way],
        )

    def step(s):
        reach = jnp.minimum(place, line - 1 - place)
        far = (s + 1) // 2
        swing = jnp.where(s % 2 == 1, place + far, place - far)
        rest = jnp.where(2 * place < line - 1, s, line - 1 - s)
        there = jnp.where(s <= 2 * reach, swing, rest)
        return there, there > place

    def forwards(above):
        return (above & can_down) | (jnp.logical_not(above) & can_up)

    def block_of(there, other):
        return there * PAIR + (1 - side if other else side)

    def relay(s, kind, other):
        there, above = step(s)
        block = block_of(there, other)

        @pl.when(forwards(above))
        def _():
            w_copy(kind, block, 2).wait_recv()
            pl.when(above & can_down)(w_copy(kind, block, 0).start)
            pl.when(jnp.logical_not(above) & can_up)(w_copy(kind, block, 1).start)

    def settle(s, kind, other):
        there, above = step(s)
        block = block_of(there, other)
        pl.when(jnp.logical_not(forwards(above)))(w_copy(kind, block, 2).wait_recv)

    kv_low = remote(
        band.at[pl.ds(WINDOW, WINDOW), :],
        band.at[pl.ds(WINDOW + tok, WINDOW), :],
        kv_send.at[0],
        kv_recv.at[1],
        sp=me - 1,
    )
    kv_high = remote(
        band.at[pl.ds(tok, WINDOW), :],
        band.at[pl.ds(0, WINDOW), :],
        kv_send.at[1],
        kv_recv.at[0],
        sp=me + 1,
    )

    def shares(index, half=None):
        if half is None:
            return pl.ds(pl.multiple_of(index * share, share), share)
        size = share // 2
        return pl.ds(pl.multiple_of(index * share + half * size, size), size)

    own_local = [
        pltpu.make_async_copy(wo_ref, wo.at[my_tp], local_sem.at[1]),
        pltpu.make_async_copy(res_ref.at[shares(my_tp), :], mid, local_sem.at[2]),
    ] + [
        pltpu.make_async_copy(w_part(kind, side), w_slot(kind, me), local_sem.at[3 + kind])
        for kind in range(3)
    ]

    def wo_copy(k, own=True):
        slot = wo.at[my_tp if own else across]
        return remote(
            wo_ref if own else slot,
            slot,
            wo_send.at[k],
            wo_recv.at[my_tp if own else across],
            tp=(buddy, across, buddy)[k],
        )

    def arrived(ref, recv, source):
        slot = ref.at[source]
        return remote(slot, slot, wo_send.at[0], recv.at[source], tp=buddy)

    pl.when(has_low)(kv_low.start)
    pl.when(has_high)(kv_high.start)
    for copy in own_local:
        copy.start()
    for kind in range(2):
        w_copy(kind, me, 2, True).start()
        pl.when(can_down)(w_copy(kind, me, 0, True).start)
        pl.when(can_up)(w_copy(kind, me, 1, True).start)
    w_copy(2, me, 2, True).start()
    wo_copy(1).start()
    wo_copy(0).start()

    for ref, taps in ((tg_ref, tapg), (tv_ref, tapv)):
        taps[...] = jnp.where(side == 0, ref[:, 0:wide], ref[:, wide : 2 * wide]).astype(F32)

    blank = jnp.zeros((WINDOW, band.shape[1]), BF16)

    @pl.when(jnp.logical_not(has_low))
    def _():
        band[pl.ds(0, WINDOW), :] = blank

    @pl.when(jnp.logical_not(has_high))
    def _():
        band[pl.ds(WINDOW + tok, WINDOW), :] = blank

    for i in range(1, tok // WINDOW - 1):
        own_band(i)
    for copy in early_local:
        copy.wait()
    pl.when(has_low)(kv_high.wait_recv)
    pl.when(has_high)(kv_low.wait_recv)
    heads = q.shape[1] // HD
    span = 3 * WINDOW
    steps = tok + 2 * WINDOW
    total = tok * sp
    lane = lax.broadcasted_iota(jnp.int32, (WINDOW, 2 * HD), 1)
    early = lane % HD < HD // 2
    low = lane < HD

    def turn(field, start):
        rows = pl.ds(start, WINDOW)
        base_cos = table[pl.ds(2 * steps + me, 1), :]
        base_sin = table[pl.ds(2 * steps + sp + me, 1), :]
        near_cos = table[rows, :]
        near_sin = table[pl.ds(pl.multiple_of(steps + start, WINDOW), WINDOW), :]
        cosine = base_cos * near_cos - base_sin * near_sin
        sine = base_sin * near_cos + base_cos * near_sin
        ahead = pltpu.roll(field, 2 * HD - HD // 2, 1)
        behind = pltpu.roll(field, HD // 2, 1)
        return field * cosine + jnp.where(early, -ahead, behind) * sine

    def turn_keys(i, carry):
        start = pl.multiple_of(i * WINDOW, WINDOW)
        field = band[pl.ds(start, WINDOW), :].astype(F32)
        field = jnp.where(low, turn(field, start), field)
        key_value[pl.ds(start, WINDOW), :] = field.astype(BF16)
        value_key[pl.ds(start, WINDOW), :] = pltpu.roll(field, HD, 1).astype(BF16)
        return carry

    lax.fori_loop(0, tok // WINDOW + 2, turn_keys, 0)

    def att_copy(k):
        peer = (corner, across, buddy)[k]
        return remote(
            att.at[shares(peer), :],
            att_all.at[my_tp],
            att_send.at[k],
            att_recv.at[my_tp],
            tp=peer,
        )

    per = share // WINDOW

    def attend(i, carry):
        k = i // per
        target = jnp.where(
            k == 0, corner, jnp.where(k == 1, across, jnp.where(k == 2, buddy, my_tp))
        )
        start = pl.multiple_of(target * share + i % per * WINDOW, WINDOW)
        straight = key_value[pl.ds(start, span), :]
        crossed = value_key[pl.ds(start, span), :]
        row = lax.broadcasted_iota(jnp.int32, (WINDOW, span), 0)
        col = lax.broadcasted_iota(jnp.int32, (WINDOW, span), 1)
        key_pos = col + (me * tok - WINDOW + start)
        valid = (col >= row) & (col <= row + 2 * WINDOW) & (key_pos >= 0) & (key_pos < total)

        def head(query, sink, keys, values):
            scores = lax.dot_general(
                query, keys, (((1,), (1,)), ((), ())), preferred_element_type=F32
            )
            scores = jnp.where(valid, scores, -1e30)
            top = jnp.maximum(jnp.max(scores, axis=-1, keepdims=True), sink)
            weights = jnp.exp(scores - top)
            denom = jnp.sum(weights, axis=-1, keepdims=True) + jnp.exp(sink - top)
            probs = (weights * (1.0 / denom)).astype(BF16)
            return jnp.dot(probs, values, preferred_element_type=F32)

        for h in range(0, heads, 2):
            lanes = pl.ds(h * HD, 2 * HD)
            field = q[pl.ds(start, WINDOW), lanes].astype(F32)
            field = turn(field, pl.multiple_of(start + WINDOW, WINDOW)) * HD**-0.5
            even = head(
                jnp.where(low, field, 0.0).astype(BF16), sink_ref[h], straight, crossed
            )
            odd = head(
                jnp.where(low, 0.0, field).astype(BF16), sink_ref[h + 1], crossed, straight
            )
            att[pl.ds(start, WINDOW), lanes] = jnp.where(low, even, odd).astype(BF16)
        for n in range(tp - 1):
            pl.when(i == per * (n + 1) - 1)(att_copy(n).start)

        @pl.when(i == per * 2 - 1)
        def _():
            for kind in range(2):
                w_copy(kind, mate, 2).wait_recv()
                pl.when(can_down)(w_copy(kind, mate, 0).start)
                pl.when(can_up)(w_copy(kind, mate, 1).start)
            for kind in range(2):
                for s in (1, 2):
                    if s < line:
                        relay(s, kind, False)

        return carry

    lax.fori_loop(0, tok // WINDOW, attend, 0)
    att_all[my_tp] = att[shares(my_tp), :]
    for kind in range(2):
        for s in (1, 2):
            if s < line:
                relay(s, kind, True)
    arrived(wo, wo_recv, across).wait_recv()
    wo_copy(2, False).start()

    own_local[0].wait()
    own_local[1].wait()
    for source in (buddy, across, corner):
        if source is not across:
            arrived(wo, wo_recv, source).wait_recv()
        arrived(att_all, att_recv, source).wait_recv()
    piece = 512
    mine = side * tp + my_tp
    squares = jnp.zeros((share, 1), F32)
    for c in range(0, width, piece):
        acc = jnp.zeros((share, piece), F32)
        for k in range(tp):
            term = jnp.dot(att_all[k], wo[k, :, pl.ds(c, piece)], preferred_element_type=F32)
            acc = acc + term.astype(BF16).astype(F32)
        new = (mid[:, pl.ds(c, piece)].astype(F32) + acc).astype(BF16)
        mid[:, pl.ds(c, piece)] = new
        field = new.astype(F32)
        squares = squares + jnp.sum(field * field, axis=-1, keepdims=True)
    scale = lax.rsqrt(squares * (1.0 / width) + EPS)
    for c in range(0, width, piece):
        field = mid[:, pl.ds(c, piece)].astype(F32)
        normed[shares(mine), pl.ds(c, piece)] = (
            field * scale * gain_ref[:, pl.ds(c, piece)]
        ).astype(BF16)

    from_mate = (1 - side) * tp + my_tp
    from_across = side * tp + across
    from_corner = side * tp + corner
    diagonal = (1 - side) * tp + across
    rows_sent = [
        (mine, None, "buddy"),
        (mine, None, "mate"),
        (mine, None, "across"),
        (from_mate, None, "buddy"),
        (from_mate, 0, "across"),
        (from_across, None, "buddy"),
        (from_across, 1, "mate"),
        (diagonal, 0, "buddy"),
        (diagonal, 1, "buddy"),
    ]

    def n_copy(k):
        index, half, goal = rows_sent[k]
        slot = normed.at[shares(index, half), :]
        where = {"sp": mate} if goal == "mate" else {"tp": buddy if goal == "buddy" else across}
        return remote(slot, slot, n_send.at[k], n_recv.at[index, half or 0], **where)

    def n_wait(index, half=None):
        slot = normed.at[shares(index, half), :]
        remote(slot, slot, n_send.at[0], n_recv.at[index, half or 0], tp=buddy).wait_recv()

    for k in (1, 2, 0):
        n_copy(k).start()

    def relay_all(steps, kinds, other):
        for s in steps:
            if s < line:
                for kind in kinds:
                    relay(s, kind, other)

    relay_all(range(3, line), (0, 1), False)
    relay_all(range(3, line), (0, 1), True)

    w_copy(2, mate, 2).wait_recv()
    inner_down = can_down & jnp.logical_not(end_down)
    inner_up = can_up & jnp.logical_not(end_up)

    def start_down(down, up, other):
        block = mate if other else me
        pl.when(down)(w_copy(2, block, 0, not other).start)
        pl.when(up)(w_copy(2, block, 1, not other).start)

    start_down(can_down, can_up, False)
    start_down(inner_down, inner_up, True)

    last_there, _ = step(line - 1)
    plane = PAIR * depth
    tail = pl.ds(pl.multiple_of(last_there * plane, plane), plane)
    main_start = jnp.where(last_there == 0, plane, 0)
    main = pl.ds(pl.multiple_of(main_start, plane), (line - 1) * plane)
    tile = share
    tiles = group // tile

    def up_main(i):
        left = normed[shares(i), main]
        rows = pl.ds(pl.multiple_of(i * tile + EDGE, EDGE), tile)
        for weight, dest in ((wg, upg), (wv, upv)):
            dest[rows, :] = jnp.dot(left, weight[main, :], preferred_element_type=F32)

    def up_tail(i):
        left = normed[shares(i), tail]
        rows = pl.ds(pl.multiple_of(i * tile + EDGE, EDGE), tile)
        for weight, dest in ((wg, upg), (wv, upv)):
            term = jnp.dot(left, weight[tail, :], preferred_element_type=F32)
            dest[rows, :] = (dest[rows, :] + term).astype(BF16).astype(F32)

    def settle_up(s):
        for other in (False, True):
            for kind in range(2):
                settle(s, kind, other)

    for s in range(1, line - 1):
        settle_up(s)
    for kind in range(2):
        own_local[2 + kind].wait()
    up_main(mine)
    n_wait(side * tp + buddy)
    up_main(side * tp + buddy)
    n_wait(from_mate)
    n_copy(4).start()
    n_copy(3).start()
    n_wait(from_across)
    n_copy(6).start()
    n_copy(5).start()
    up_main(from_mate)
    up_main(from_across)
    n_wait((1 - side) * tp + buddy)
    up_main((1 - side) * tp + buddy)
    n_wait(from_corner)
    up_main(from_corner)
    for half in range(2):
        n_wait(diagonal, half)
        n_copy(7 + half).start()
    up_main(diagonal)
    for half in range(2):
        n_wait((1 - side) * tp + corner, half)
    up_main((1 - side) * tp + corner)
    settle_up(line - 1)

    def up_step(i, carry):
        up_tail(i)
        return carry

    def edge_low(kind):
        ref = (upg, upv)[kind]
        return remote(
            ref.at[pl.ds(EDGE, EDGE), :],
            ref.at[pl.ds(EDGE + group, EDGE), :],
            edge_send.at[0, kind],
            edge_recv.at[1, kind],
            sp=me - PAIR,
        )

    def edge_high(kind):
        ref = (upg, upv)[kind]
        return remote(
            ref.at[pl.ds(group, EDGE), :],
            ref.at[pl.ds(0, EDGE), :],
            edge_send.at[1, kind],
            edge_recv.at[0, kind],
            sp=me + PAIR,
        )

    up_tail(0)
    up_tail(tiles - 1)
    for kind in range(2):
        pl.when(can_down)(edge_low(kind).start)
        pl.when(can_up)(edge_high(kind).start)
    start_down(can_down & end_down, can_up & end_up, True)
    relay_all((1, 2), (2,), False)
    relay_all((1, 2), (2,), True)
    lax.fori_loop(1, tiles - 1, up_step, 0)

    none = jnp.zeros((EDGE, wide), F32)

    @pl.when(jnp.logical_not(can_down))
    def _():
        upg[pl.ds(0, EDGE), :] = none
        upv[pl.ds(0, EDGE), :] = none

    @pl.when(jnp.logical_not(can_up))
    def _():
        upg[pl.ds(EDGE + group, EDGE), :] = none
        upv[pl.ds(EDGE + group, EDGE), :] = none

    for kind in range(2):
        pl.when(can_down)(edge_high(kind).wait_recv)
        pl.when(can_up)(edge_low(kind).wait_recv)

    def gate(i, carry):
        base = pl.multiple_of(i * WINDOW, WINDOW)
        for c in range(0, wide, 256):
            lanes = pl.ds(c, 256)

            def convolve(ref, taps):
                field = ref[pl.ds(base, WINDOW + 2 * EDGE), lanes]
                return (
                    field[EDGE - 1 : EDGE - 1 + WINDOW] * taps[0:1, lanes]
                    + field[EDGE : EDGE + WINDOW] * taps[1:2, lanes]
                    + field[EDGE + 1 : EDGE + 1 + WINDOW] * taps[2:3, lanes]
                )

            g = convolve(upg, tapg)
            v = convolve(upv, tapv)
            hidden[pl.ds(base, WINDOW), lanes] = (g / (1.0 + jnp.exp(-g)) * v).astype(BF16)
        return carry

    lax.fori_loop(0, group // WINDOW, gate, 0)
    relay_all(range(3, line), (2,), False)


    def r_copy(k, block):
        src, dst = (
            (terms.at[block, :, :, 1 - core], near.at[block]),
            (pair_sum.at[block, 0, 1 - side], first_x.at[block]),
            (pair_sum.at[block, 1, :, 1 - row_y], first_y.at[block]),
            (sum_x.at[block], last_x.at[block]),
            (sum_y.at[block], last_y.at[block]),
        )[k]
        where = ({"tp": buddy}, {"sp": mate}, {"tp": across}, {"tp": across}, {"sp": mate})[k]
        return remote(src, dst, r_send.at[k, block], r_recv.at[k, block], **where)

    def block_at(j):
        there, _ = step(j // 2)
        return there * PAIR + jnp.where(j % 2 == 0, side, 1 - side)

    def produce(j):
        block = block_at(j)

        @pl.when(j == 0)
        def _():
            own_local[4].wait()

        @pl.when(j == 2)
        def _():
            relay_all(range(3, line), (2,), True)

        @pl.when(j > 1)
        def _():
            there, above = step(j // 2)
            pl.when(jnp.logical_not(forwards(above)))(w_copy(2, block, 2).wait_recv)

        def part(i, carry):
            rows = pl.ds(pl.multiple_of(i * 2 * share, 2 * share), 2 * share)
            term = jnp.dot(hidden[rows, :], wd[block], preferred_element_type=F32)
            terms[block, i // 2, i % 2] = term.astype(BF16).reshape(2, share, cols)
            return carry

        lax.fori_loop(0, group // (2 * share), part, 0)
        r_copy(0, block).start()

    def pass_first(j):
        block = block_at(j)
        r_copy(0, block).wait_recv()
        for x in range(PAIR):
            for y in range(tp // 2):
                both = terms[block, x, y, core].astype(F32) + near[block, x, y].astype(F32)
                pair_sum[block, 0, x, y] = both[:, :lane_half].astype(BF16)
                pair_sum[block, 1, x, y] = both[:, lane_half:].astype(BF16)
        r_copy(1, block).start()
        r_copy(2, block).start()

    def pass_second(j):
        block = block_at(j)
        r_copy(1, block).wait_recv()
        both = pair_sum[block, 0, side, 1 - row_y].astype(F32)
        sum_x[block] = (both + first_x[block, 1 - row_y].astype(F32)).astype(BF16)
        r_copy(3, block).start()
        r_copy(2, block).wait_recv()
        both = pair_sum[block, 1, 1 - side, row_y].astype(F32)
        sum_y[block] = (both + first_y[block, 1 - side].astype(F32)).astype(BF16)
        r_copy(4, block).start()

    lag = 3

    def down(j, carry):
        pl.when(j >= lag)(lambda: pass_second(j - lag))
        pl.when((j > 0) & (j < sp + 1))(lambda: pass_first(j - 1))
        pl.when(j < sp)(lambda: produce(j))
        return carry

    lax.fori_loop(0, sp + lag, down, 0)

    for block in range(sp):
        r_copy(3, block).wait_recv()
        r_copy(4, block).wait_recv()
        for half in range(2):
            first = first_x[block, row_y] if half == 0 else first_y[block, side]
            last = last_x[block] if half == 0 else last_y[block]
            lanes = pl.ds(block * cols + half * lane_half, lane_half)
            acc = mid[:, lanes].astype(F32) + pair_sum[block, half, side, row_y].astype(F32)
            acc = acc + first.astype(F32) + last.astype(F32)
            out_ref[:, lanes] = acc.astype(BF16)

    for kind in range(3):
        w_copy(kind, me, 2, True).wait_send()
        for block in (me, mate):
            pl.when(can_down)(w_copy(kind, block, 0).wait_send)
            pl.when(can_up)(w_copy(kind, block, 1).wait_send)

    def drain(s, carry):
        there, above = step(s)
        for kind in range(3):
            for other in (False, True):
                block = block_of(there, other)
                pl.when(above & can_down)(w_copy(kind, block, 0).wait_send)
                pl.when(jnp.logical_not(above) & can_up)(w_copy(kind, block, 1).wait_send)
        return carry

    lax.fori_loop(1, line, drain, 0)
    for k in range(tp - 1):
        wo_copy(k, k < 2).wait_send()
        att_copy(k).wait_send()
    for k in range(len(rows_sent)):
        n_copy(k).wait_send()
    pl.when(has_low)(kv_low.wait_send)
    pl.when(has_high)(kv_high.wait_send)
    for kind in range(2):
        pl.when(can_down)(edge_low(kind).wait_send)
        pl.when(can_up)(edge_high(kind).wait_send)

    def drain_sums(block, carry):
        for k in range(5):
            r_copy(k, block).wait_send()
        return carry

    lax.fori_loop(0, sp, drain_sums, 0)


def kernel_shards(
    sp,
    tp,
    residual,
    query,
    key,
    value,
    sink,
    norm_gain,
    w_out,
    w_gate,
    w_value,
    conv_gate,
    conv_value,
    w_down,
):
    tok, width = residual.shape
    depth, hid = w_gate.shape
    cols = w_down.shape[1]
    heads = query.shape[1] // HD
    share = tok // tp
    wide = hid // PAIR
    group = PAIR * tok
    inverse = THETA ** (-(np.arange(2 * HD) % (HD // 2)) * 2.0 / HD)
    local = (np.arange(tok + 2 * WINDOW) - WINDOW)[:, None] * inverse[None, :]
    first = (np.arange(sp) * tok)[:, None] * inverse[None, :]
    table = np.concatenate([np.cos(local), np.sin(local), np.cos(first), np.sin(first)])
    vmem = pl.BlockSpec(memory_space=pltpu.VMEM)
    smem = pl.BlockSpec(memory_space=pltpu.SMEM)
    anywhere = pl.BlockSpec(memory_space=pl.ANY)
    dma = pltpu.SemaphoreType.DMA
    return pl.pallas_call(
        functools.partial(layer_kernel, sp, tp),
        out_shape=pltpu.VMEM((tok // tp, width), BF16),
        in_specs=[anywhere, vmem, vmem, anywhere, smem, anywhere, vmem]
        + [anywhere] * 3
        + [vmem] * 2
        + [anywhere],
        out_specs=vmem,
        scratch_shapes=[
            pltpu.VMEM(query.shape, BF16),
            pltpu.VMEM(table.shape, F32),
            pltpu.VMEM((tok + 2 * WINDOW, 2 * HD), BF16),
            pltpu.VMEM((tok + 2 * WINDOW, 2 * HD), BF16),
            pltpu.VMEM((tok + 2 * WINDOW, 2 * HD), BF16),
            pltpu.VMEM((tok, heads * HD), BF16),
            pltpu.VMEM((tp, share, heads * HD), BF16),
            pltpu.VMEM((tp,) + w_out.shape, BF16),
            pltpu.VMEM((sp * depth, wide), BF16),
            pltpu.VMEM((sp * depth, wide), BF16),
            pltpu.VMEM((sp, wide, cols), BF16),
            pltpu.VMEM((share, width), BF16),
            pltpu.VMEM((group, width), BF16),
            pltpu.VMEM((group + 2 * EDGE, wide), F32),
            pltpu.VMEM((group + 2 * EDGE, wide), F32),
            pltpu.VMEM((group, wide), BF16),
            pltpu.VMEM((sp, PAIR, tp // 2, 2, share, cols), BF16),
            pltpu.VMEM((sp, PAIR, tp // 2, share, cols), BF16),
            pltpu.VMEM((sp, 2, PAIR, tp // 2, share, cols // 2), BF16),
            pltpu.VMEM((sp, tp // 2, share, cols // 2), BF16),
            pltpu.VMEM((sp, PAIR, share, cols // 2), BF16),
            pltpu.VMEM((sp, share, cols // 2), BF16),
            pltpu.VMEM((sp, share, cols // 2), BF16),
            pltpu.VMEM((sp, share, cols // 2), BF16),
            pltpu.VMEM((sp, share, cols // 2), BF16),
            pltpu.VMEM((3, wide), F32),
            pltpu.VMEM((3, wide), F32),
            dma((7,)),
            dma((3, sp, 3)),
            dma((3, sp)),
            dma((tp - 1,)),
            dma((tp,)),
            dma((tp - 1,)),
            dma((tp,)),
            dma((2,)),
            dma((2,)),
            dma((2, 2)),
            dma((2, 2)),
            dma((9,)),
            dma((PAIR * tp, 2)),
            dma((5, sp)),
            dma((5, sp)),
        ],
        compiler_params=pltpu.CompilerParams(
            collective_id=0, has_side_effects=True, vmem_limit_bytes=62 * 1000 * 1000
        ),
        name="layer",
    )(
        query,
        key.T,
        value.T,
        jnp.asarray(table, F32),
        sink,
        residual,
        norm_gain.reshape(1, -1),
        w_out,
        w_gate,
        w_value,
        conv_gate,
        conv_value,
        w_down,
    )


def solution(mesh):
    sp, tp = mesh.shape["sp"], mesh.shape["tp"]

    def shards(*args):
        if args[11].shape[1] % 256 or sp % PAIR or tp != 4 or args[2].shape[1] != HD:
            return plain_shards(*args)
        return kernel_shards(sp, tp, *args)

    return jax.shard_map(
        shards,
        mesh=mesh,
        in_specs=(
            P("sp", None),
            P("sp", "tp"),
            P("sp", "tp"),
            P("sp", "tp"),
            P("tp"),
            P(),
            P("tp", None),
            P("sp", "tp"),
            P("sp", "tp"),
            P(None, "tp"),
            P(None, "tp"),
            P("tp", "sp"),
        ),
        out_specs=P(("sp", "tp"), None),
        check_vma=False,
    )
```

```python
import functools

import jax
import jax.numpy as jnp
import numpy as np
from jax import lax
from jax.experimental import pallas as pl
from jax.experimental.pallas import tpu as pltpu
from jax.sharding import PartitionSpec as P

HD = 64
WINDOW = 128


THETA = 10000.0
EPS = 1e-06


def extended(block, sides, width):
    for axis, dim in sides:
        count = lax.axis_size(axis)
        forward = [(i, i + 1) for i in range(count - 1)]
        backward = [(target, source) for source, target in forward]
        low = lax.ppermute(
            lax.slice_in_dim(block, block.shape[dim] - width, None, axis=dim), axis, forward
        )
        high = lax.ppermute(lax.slice_in_dim(block, 0, width, axis=dim), axis, backward)
        block = jnp.concatenate([low, block, high], axis=dim)
    return block


def rotate(field, positions):
    count = field.shape[0]
    parts = field.astype(jnp.float32).reshape(count, -1, HD)
    inverse = 1.0 / THETA ** (jnp.arange(0, HD, 2, dtype=jnp.float32) / HD)
    angle = positions[:, None] * inverse[None, :]
    cosine = jnp.cos(angle)[:, None, :]
    sine = jnp.sin(angle)[:, None, :]
    first = parts[..., : HD // 2]
    second = parts[..., HD // 2 :]
    turned = jnp.concatenate(
        [first * cosine - second * sine, second * cosine + first * sine], axis=-1
    )
    return turned.reshape(count, -1).astype(jnp.bfloat16)


def band_attention(queries, keys, values, sinks, start, total):
    count = queries.shape[0]
    blocks = count // WINDOW
    kv_local = keys.shape[1] // HD
    group = queries.shape[1] // (kv_local * HD)
    query_blocks = queries.reshape(blocks, WINDOW, kv_local, group, HD)
    key_band = jnp.concatenate(
        [
            keys[i * WINDOW : i * WINDOW + count].reshape(blocks, WINDOW, kv_local, HD)
            for i in range(3)
        ],
        axis=1,
    )
    value_band = jnp.concatenate(
        [
            values[i * WINDOW : i * WINDOW + count].reshape(blocks, WINDOW, kv_local, HD)
            for i in range(3)
        ],
        axis=1,
    )
    scores = jnp.einsum(
        "nqkgd,njkd->nkgqj", query_blocks, key_band, preferred_element_type=jnp.float32
    ) * HD ** (-0.5)
    block_ids = jnp.arange(blocks, dtype=jnp.int32)[:, None]
    query_pos = start + block_ids * WINDOW + jnp.arange(WINDOW, dtype=jnp.int32)[None, :]
    key_pos = start - WINDOW + block_ids * WINDOW + jnp.arange(3 * WINDOW, dtype=jnp.int32)[None, :]
    valid = (
        (key_pos[:, None, :] >= 0)
        & (key_pos[:, None, :] < total)
        & (jnp.abs(query_pos[:, :, None] - key_pos[:, None, :]) <= WINDOW)
    )
    scores = jnp.where(valid[:, None, None], scores, -1e30)
    sink_col = sinks.reshape(1, kv_local, group, 1, 1)
    top = jnp.maximum(jnp.max(scores, axis=-1, keepdims=True), sink_col)
    weights = jnp.exp(scores - top)
    denom = jnp.sum(weights, axis=-1, keepdims=True) + jnp.exp(sink_col - top)
    probs = (weights / denom).astype(jnp.bfloat16)
    out = jnp.einsum("nkgqj,njkd->nqkgd", probs, value_band, preferred_element_type=jnp.float32)
    return out.reshape(count, kv_local * group * HD).astype(jnp.bfloat16)


def rmsnorm(field, gain):
    wide = field.astype(jnp.float32)
    scale = lax.rsqrt(jnp.mean(wide * wide, axis=-1, keepdims=True) + EPS)
    return (wide * scale * gain).astype(jnp.bfloat16)


def plain_shards(
    residual,
    query,
    key,
    value,
    sink,
    norm_gain,
    w_out,
    w_gate,
    w_value,
    conv_gate,
    conv_value,
    w_down,
):
    tok_rows = query.shape[0]
    offset = lax.axis_index("sp") * tok_rows
    total = tok_rows * lax.axis_size("sp")
    share = tok_rows // lax.axis_size("tp")
    tp_index = lax.axis_index("tp")
    positions = (offset + jnp.arange(tok_rows, dtype=jnp.int32)).astype(jnp.float32)
    turned_query = rotate(query, positions)
    turned_key = rotate(key, positions)
    key_width = key.shape[1]
    band = jnp.concatenate([turned_key, value], axis=1)
    edged = extended(band, (("sp", 0),), WINDOW)
    attended = band_attention(
        turned_query, edged[:, :key_width], edged[:, key_width:], sink, offset, total
    )
    partial_value = jnp.dot(attended, w_out, preferred_element_type=jnp.float32)
    mix_full = lax.psum(partial_value.astype(jnp.bfloat16), "tp").astype(jnp.float32)
    mid_full = (residual.astype(jnp.float32) + mix_full).astype(jnp.bfloat16)
    normed = rmsnorm(mid_full, norm_gain)
    mid_rows = lax.dynamic_slice_in_dim(mid_full, tp_index * share, share, 0)
    gate_full, value_full = (
        lax.all_gather(w_gate, "sp", axis=0, tiled=True),
        lax.all_gather(w_value, "sp", axis=0, tiled=True),
    )
    gate_up = jnp.dot(normed, gate_full, preferred_element_type=jnp.float32).astype(jnp.bfloat16)
    value_up = jnp.dot(normed, value_full, preferred_element_type=jnp.float32).astype(jnp.bfloat16)
    hidden_width = gate_up.shape[1]
    stacked = jnp.concatenate([gate_up, value_up], axis=1)
    edged_up = extended(stacked, (("sp", 0),), 1).astype(jnp.float32)
    taps = jnp.concatenate([conv_gate, conv_value], axis=1).astype(jnp.float32)
    convolved = edged_up[:-2] * taps[0] + edged_up[1:-1] * taps[1] + edged_up[2:] * taps[2]
    hidden = (jax.nn.silu(convolved[:, :hidden_width]) * convolved[:, hidden_width:]).astype(
        jnp.bfloat16
    )
    terms = jnp.dot(
        hidden, lax.all_gather(w_down, "sp", axis=1, tiled=True), preferred_element_type=jnp.float32
    )
    ffn_rows = lax.psum_scatter(
        terms.astype(jnp.bfloat16), "tp", scatter_dimension=0, tiled=True
    ).astype(jnp.float32)
    return (mid_rows.astype(jnp.float32) + ffn_rows).astype(jnp.bfloat16)


F32 = jnp.float32
BF16 = jnp.bfloat16
PAIR = 2
EDGE = 8


def layer_kernel(
    sp,
    tp,
    q_ref,
    k_ref,
    v_ref,
    table_ref,
    sink_ref,
    res_ref,
    gain_ref,
    wo_ref,
    wg_ref,
    wv_ref,
    tg_ref,
    tv_ref,
    wd_ref,
    out_ref,
    q,
    table,
    band,
    key_value,
    value_key,
    att,
    att_all,
    wo,
    wg,
    wv,
    wd,
    mid,
    normed,
    upg,
    upv,
    hidden,
    terms,
    near,
    pair_sum,
    first_x,
    first_y,
    sum_x,
    sum_y,
    last_x,
    last_y,
    tapg,
    tapv,
    local_sem,
    w_send,
    w_recv,
    wo_send,
    wo_recv,
    att_send,
    att_recv,
    kv_send,
    kv_recv,
    edge_send,
    edge_recv,
    n_send,
    n_recv,
    r_send,
    r_recv,
):
    me = lax.axis_index("sp")
    my_tp = lax.axis_index("tp")
    tok = q.shape[0]
    share, width = mid.shape
    group = normed.shape[0]
    line = sp // PAIR
    place = me // PAIR
    side = me % PAIR
    mate = place * PAIR + (1 - side)
    depth = wg_ref.shape[0]
    wide = wg.shape[1]
    cols = wd_ref.shape[1]
    unit = cols // PAIR
    row_half = share // 2
    downs = tuple(range(2, 2 + PAIR))
    has_low = me > 0
    has_high = me < sp - 1
    can_down = place > 0
    can_up = place < line - 1
    end_down = place == 1
    end_up = place == line - 2
    row_y = my_tp // 2
    core = my_tp % 2
    buddy = my_tp + 1 - 2 * core
    across = lax.rem(my_tp + 2, tp)
    corner = lax.rem(buddy + 2, tp)

    def remote(src, dst, send, recv, **where):
        return pltpu.make_async_remote_copy(
            src_ref=src,
            dst_ref=dst,
            send_sem=send,
            recv_sem=recv,
            device_id=where,
            device_id_type=pl.DeviceIdType.MESH,
        )

    barrier = pltpu.get_barrier_semaphore()

    def greet(**where):
        pl.semaphore_signal(
            barrier, inc=1, device_id=where, device_id_type=pl.DeviceIdType.MESH
        )

    def own_band(i):
        lanes = pl.ds(i * WINDOW, WINDOW)
        pair = jnp.concatenate([k_ref[:, lanes], v_ref[:, lanes]], axis=0)
        band[pl.ds((i + 1) * WINDOW, WINDOW), :] = pair.astype(F32).T.astype(BF16)

    greet(sp=mate)
    for peer in (buddy, across, corner):
        greet(tp=peer)
    far_low = has_low & (side == 0)
    far_high = has_high & (side == PAIR - 1)
    pl.when(far_low)(lambda: greet(sp=me - 1))
    pl.when(far_high)(lambda: greet(sp=me + 1))
    pl.when(can_down)(lambda: greet(sp=me - PAIR))
    pl.when(can_up)(lambda: greet(sp=me + PAIR))
    count = tp
    for able in (far_low, far_high, can_down, can_up):
        count = count + jnp.where(able, 1, 0)
    early_local = [
        pltpu.make_async_copy(q_ref, q, local_sem.at[0]),
        pltpu.make_async_copy(table_ref, table, local_sem.at[3 + PAIR + 2]),
    ]
    for copy in early_local:
        copy.start()
    own_band(0)
    own_band(tok // WINDOW - 1)
    pl.semaphore_wait(barrier, count)

    def w_part(kind, half):
        start = pl.multiple_of(half * wide, wide)
        if kind > 1:
            return wd_ref.at[pl.ds(start, wide), pl.ds((kind - 2) * unit, unit)]
        return (wg_ref, wv_ref)[kind].at[:, pl.ds(start, wide)]

    def w_slot(kind, block):
        if kind > 1:
            return wd.at[block, :, pl.ds((kind - 2) * unit, unit)]
        return (wg, wv)[kind].at[pl.ds(pl.multiple_of(block * depth, depth), depth), :]

    def w_copy(kind, block, way, own=False):
        slot = w_slot(kind, block)
        src = w_part(kind, 1 - side if way == 2 else side) if own else slot
        return remote(
            src,
            slot,
            w_send.at[kind, block, way],
            w_recv.at[kind, block],
            sp=(me - PAIR, me + PAIR, mate)[way],
        )

    def step(s):
        reach = jnp.minimum(place, line - 1 - place)
        far = (s + 1) // 2
        swing = jnp.where(s % 2 == 1, place + far, place - far)
        rest = jnp.where(2 * place < line - 1, s, line - 1 - s)
        there = jnp.where(s <= 2 * reach, swing, rest)
        return there, there > place

    def forwards(above):
        return (above & can_down) | (jnp.logical_not(above) & can_up)

    def block_of(there, other, kind=0):
        if kind > 1:
            return there * PAIR + (1 if other else 0)
        return there * PAIR + (1 - side if other else side)

    def relay(s, kind, other):
        there, above = step(s)
        block = block_of(there, other, kind)

        @pl.when(forwards(above))
        def _():
            w_copy(kind, block, 2).wait_recv()
            pl.when(above & can_down)(w_copy(kind, block, 0).start)
            pl.when(jnp.logical_not(above) & can_up)(w_copy(kind, block, 1).start)

    def settle(s, kind, other):
        there, above = step(s)
        block = block_of(there, other, kind)
        pl.when(jnp.logical_not(forwards(above)))(w_copy(kind, block, 2).wait_recv)

    kv_low = remote(
        band.at[pl.ds(WINDOW, WINDOW), :],
        band.at[pl.ds(WINDOW + tok, WINDOW), :],
        kv_send.at[0],
        kv_recv.at[1],
        sp=me - 1,
    )
    kv_high = remote(
        band.at[pl.ds(tok, WINDOW), :],
        band.at[pl.ds(0, WINDOW), :],
        kv_send.at[1],
        kv_recv.at[0],
        sp=me + 1,
    )

    def shares(index, half=None):
        if half is None:
            return pl.ds(pl.multiple_of(index * share, share), share)
        size = share // 2
        return pl.ds(pl.multiple_of(index * share + half * size, size), size)

    own_local = [
        pltpu.make_async_copy(wo_ref, wo.at[my_tp], local_sem.at[1]),
        pltpu.make_async_copy(res_ref.at[shares(my_tp), :], mid, local_sem.at[2]),
    ] + [
        pltpu.make_async_copy(w_part(kind, side), w_slot(kind, me), local_sem.at[3 + kind])
        for kind in range(2 + PAIR)
    ]

    def wo_copy(k, own=True):
        slot = wo.at[my_tp if own else across]
        return remote(
            wo_ref if own else slot,
            slot,
            wo_send.at[k],
            wo_recv.at[my_tp if own else across],
            tp=(buddy, across, buddy)[k],
        )

    def arrived(ref, recv, source):
        slot = ref.at[source]
        return remote(slot, slot, wo_send.at[0], recv.at[source], tp=buddy)

    pl.when(has_low)(kv_low.start)
    pl.when(has_high)(kv_high.start)
    for copy in own_local:
        copy.start()
    for kind in range(2):
        w_copy(kind, me, 2, True).start()
        pl.when(can_down)(w_copy(kind, me, 0, True).start)
        pl.when(can_up)(w_copy(kind, me, 1, True).start)
    for kind in downs:
        w_copy(kind, me, 2, True).start()
    wo_copy(1).start()
    wo_copy(0).start()

    for ref, taps in ((tg_ref, tapg), (tv_ref, tapv)):
        taps[...] = jnp.where(side == 0, ref[:, 0:wide], ref[:, wide : 2 * wide]).astype(F32)

    blank = jnp.zeros((WINDOW, band.shape[1]), BF16)

    @pl.when(jnp.logical_not(has_low))
    def _():
        band[pl.ds(0, WINDOW), :] = blank

    @pl.when(jnp.logical_not(has_high))
    def _():
        band[pl.ds(WINDOW + tok, WINDOW), :] = blank

    for i in range(1, tok // WINDOW - 1):
        own_band(i)
    for copy in early_local:
        copy.wait()
    pl.when(has_low)(kv_high.wait_recv)
    pl.when(has_high)(kv_low.wait_recv)
    heads = q.shape[1] // HD
    span = 3 * WINDOW
    steps = tok + 2 * WINDOW
    total = tok * sp
    lane = lax.broadcasted_iota(jnp.int32, (WINDOW, 2 * HD), 1)
    early = lane % HD < HD // 2
    low = lane < HD

    def turn(field, start):
        rows = pl.ds(start, WINDOW)
        base_cos = table[pl.ds(2 * steps + me, 1), :]
        base_sin = table[pl.ds(2 * steps + sp + me, 1), :]
        near_cos = table[rows, :]
        near_sin = table[pl.ds(pl.multiple_of(steps + start, WINDOW), WINDOW), :]
        cosine = base_cos * near_cos - base_sin * near_sin
        sine = base_sin * near_cos + base_cos * near_sin
        ahead = pltpu.roll(field, 2 * HD - HD // 2, 1)
        behind = pltpu.roll(field, HD // 2, 1)
        return field * cosine + jnp.where(early, -ahead, behind) * sine

    def turn_keys(i, carry):
        start = pl.multiple_of(i * WINDOW, WINDOW)
        field = band[pl.ds(start, WINDOW), :].astype(F32)
        field = jnp.where(low, turn(field, start), field)
        key_value[pl.ds(start, WINDOW), :] = field.astype(BF16)
        value_key[pl.ds(start, WINDOW), :] = pltpu.roll(field, HD, 1).astype(BF16)
        return carry

    lax.fori_loop(0, tok // WINDOW + 2, turn_keys, 0)

    def att_copy(k):
        peer = (corner, across, buddy)[k]
        return remote(
            att.at[shares(peer), :],
            att_all.at[my_tp],
            att_send.at[k],
            att_recv.at[my_tp],
            tp=peer,
        )

    per = share // WINDOW

    def attend(i, carry):
        k = i // per
        target = jnp.where(
            k == 0, corner, jnp.where(k == 1, across, jnp.where(k == 2, buddy, my_tp))
        )
        start = pl.multiple_of(target * share + i % per * WINDOW, WINDOW)
        straight = key_value[pl.ds(start, span), :]
        crossed = value_key[pl.ds(start, span), :]
        row = lax.broadcasted_iota(jnp.int32, (WINDOW, span), 0)
        col = lax.broadcasted_iota(jnp.int32, (WINDOW, span), 1)
        key_pos = col + (me * tok - WINDOW + start)
        valid = (col >= row) & (col <= row + 2 * WINDOW) & (key_pos >= 0) & (key_pos < total)

        def head(query, sink, keys, values):
            scores = lax.dot_general(
                query, keys, (((1,), (1,)), ((), ())), preferred_element_type=F32
            )
            scores = jnp.where(valid, scores, -1e30)
            top = jnp.maximum(jnp.max(scores, axis=-1, keepdims=True), sink)
            weights = jnp.exp(scores - top)
            denom = jnp.sum(weights, axis=-1, keepdims=True) + jnp.exp(sink - top)
            probs = (weights * (1.0 / denom)).astype(BF16)
            return jnp.dot(probs, values, preferred_element_type=F32)

        for h in range(0, heads, 2):
            lanes = pl.ds(h * HD, 2 * HD)
            field = q[pl.ds(start, WINDOW), lanes].astype(F32)
            field = turn(field, pl.multiple_of(start + WINDOW, WINDOW)) * HD**-0.5
            even = head(
                jnp.where(low, field, 0.0).astype(BF16), sink_ref[h], straight, crossed
            )
            odd = head(
                jnp.where(low, 0.0, field).astype(BF16), sink_ref[h + 1], crossed, straight
            )
            att[pl.ds(start, WINDOW), lanes] = jnp.where(low, even, odd).astype(BF16)
        for n in range(tp - 1):
            pl.when(i == per * (n + 1) - 1)(att_copy(n).start)

        @pl.when(i == per * 2 - 1)
        def _():
            for kind in range(2):
                w_copy(kind, mate, 2).wait_recv()
                pl.when(can_down)(w_copy(kind, mate, 0).start)
                pl.when(can_up)(w_copy(kind, mate, 1).start)
            for kind in range(2):
                for s in (1, 2):
                    if s < line:
                        relay(s, kind, False)

        return carry

    lax.fori_loop(0, tok // WINDOW, attend, 0)
    att_all[my_tp] = att[shares(my_tp), :]
    for kind in range(2):
        for s in (1, 2):
            if s < line:
                relay(s, kind, True)
    arrived(wo, wo_recv, across).wait_recv()
    wo_copy(2, False).start()

    own_local[0].wait()
    own_local[1].wait()
    for source in (buddy, across, corner):
        if source is not across:
            arrived(wo, wo_recv, source).wait_recv()
        arrived(att_all, att_recv, source).wait_recv()
    piece = 512
    mine = side * tp + my_tp
    squares = jnp.zeros((share, 1), F32)
    for c in range(0, width, piece):
        acc = jnp.zeros((share, piece), F32)
        for k in range(tp):
            term = jnp.dot(att_all[k], wo[k, :, pl.ds(c, piece)], preferred_element_type=F32)
            acc = acc + term.astype(BF16).astype(F32)
        new = (mid[:, pl.ds(c, piece)].astype(F32) + acc).astype(BF16)
        mid[:, pl.ds(c, piece)] = new
        field = new.astype(F32)
        squares = squares + jnp.sum(field * field, axis=-1, keepdims=True)
    scale = lax.rsqrt(squares * (1.0 / width) + EPS)
    for c in range(0, width, piece):
        field = mid[:, pl.ds(c, piece)].astype(F32)
        normed[shares(mine), pl.ds(c, piece)] = (
            field * scale * gain_ref[:, pl.ds(c, piece)]
        ).astype(BF16)

    from_mate = (1 - side) * tp + my_tp
    from_across = side * tp + across
    from_corner = side * tp + corner
    diagonal = (1 - side) * tp + across
    rows_sent = [
        (mine, None, "buddy"),
        (mine, None, "mate"),
        (mine, None, "across"),
        (from_mate, None, "buddy"),
        (from_mate, 0, "across"),
        (from_across, None, "buddy"),
        (from_across, 1, "mate"),
        (diagonal, 0, "buddy"),
        (diagonal, 1, "buddy"),
    ]

    def n_copy(k):
        index, half, goal = rows_sent[k]
        slot = normed.at[shares(index, half), :]
        where = {"sp": mate} if goal == "mate" else {"tp": buddy if goal == "buddy" else across}
        return remote(slot, slot, n_send.at[k], n_recv.at[index, half or 0], **where)

    def n_wait(index, half=None):
        slot = normed.at[shares(index, half), :]
        remote(slot, slot, n_send.at[0], n_recv.at[index, half or 0], tp=buddy).wait_recv()

    for k in (1, 2, 0):
        n_copy(k).start()

    def relay_all(steps, kinds, other):
        for s in steps:
            if s < line:
                for kind in kinds:
                    relay(s, kind, other)

    relay_all(range(3, line), (0, 1), False)
    relay_all(range(3, line), (0, 1), True)

    for kind in downs:
        w_copy(kind, mate, 2).wait_recv()
    inner_down = can_down & jnp.logical_not(end_down)
    inner_up = can_up & jnp.logical_not(end_up)

    def start_down(down, up, x):
        for kind in downs:
            for own in (True, False):
                here = (side == x) if own else (side != x)
                block = me if own else mate
                pl.when(down & here)(w_copy(kind, block, 0, own).start)
                pl.when(up & here)(w_copy(kind, block, 1, own).start)

    start_down(can_down, can_up, 0)
    start_down(inner_down, inner_up, 1)

    last_there, _ = step(line - 1)
    plane = PAIR * depth
    tail = pl.ds(pl.multiple_of(last_there * plane, plane), plane)
    main_start = jnp.where(last_there == 0, plane, 0)
    main = pl.ds(pl.multiple_of(main_start, plane), (line - 1) * plane)
    tile = share
    tiles = group // tile

    def up_main(i):
        left = normed[shares(i), main]
        rows = pl.ds(pl.multiple_of(i * tile + EDGE, EDGE), tile)
        for weight, dest in ((wg, upg), (wv, upv)):
            dest[rows, :] = jnp.dot(left, weight[main, :], preferred_element_type=F32)

    def up_tail(i):
        left = normed[shares(i), tail]
        rows = pl.ds(pl.multiple_of(i * tile + EDGE, EDGE), tile)
        for weight, dest in ((wg, upg), (wv, upv)):
            term = jnp.dot(left, weight[tail, :], preferred_element_type=F32)
            dest[rows, :] = (dest[rows, :] + term).astype(BF16).astype(F32)

    def settle_up(s):
        for other in (False, True):
            for kind in range(2):
                settle(s, kind, other)

    for s in range(1, line - 1):
        settle_up(s)
    for kind in range(2):
        own_local[2 + kind].wait()
    up_main(mine)
    n_wait(side * tp + buddy)
    up_main(side * tp + buddy)
    n_wait(from_mate)
    n_copy(4).start()
    n_copy(3).start()
    n_wait(from_across)
    n_copy(6).start()
    n_copy(5).start()
    up_main(from_mate)
    up_main(from_across)
    n_wait((1 - side) * tp + buddy)
    up_main((1 - side) * tp + buddy)
    n_wait(from_corner)
    up_main(from_corner)
    for half in range(2):
        n_wait(diagonal, half)
        n_copy(7 + half).start()
    up_main(diagonal)
    for half in range(2):
        n_wait((1 - side) * tp + corner, half)
    up_main((1 - side) * tp + corner)
    settle_up(line - 1)

    def up_step(i, carry):
        up_tail(i)
        return carry

    def edge_low(kind):
        ref = (upg, upv)[kind]
        return remote(
            ref.at[pl.ds(EDGE, EDGE), :],
            ref.at[pl.ds(EDGE + group, EDGE), :],
            edge_send.at[0, kind],
            edge_recv.at[1, kind],
            sp=me - PAIR,
        )

    def edge_high(kind):
        ref = (upg, upv)[kind]
        return remote(
            ref.at[pl.ds(group, EDGE), :],
            ref.at[pl.ds(0, EDGE), :],
            edge_send.at[1, kind],
            edge_recv.at[0, kind],
            sp=me + PAIR,
        )

    up_tail(0)
    up_tail(tiles - 1)
    for kind in range(2):
        pl.when(can_down)(edge_low(kind).start)
        pl.when(can_up)(edge_high(kind).start)
    start_down(can_down & end_down, can_up & end_up, 1)
    for s in (1, 2):
        for other in (False, True):
            relay_all((s,), downs, other)

    def gate(base):
        for c in range(0, wide, 256):
            lanes = pl.ds(c, 256)

            def convolve(ref, taps):
                field = ref[pl.ds(base, WINDOW + 2 * EDGE), lanes]
                return (
                    field[EDGE - 1 : EDGE - 1 + WINDOW] * taps[0:1, lanes]
                    + field[EDGE : EDGE + WINDOW] * taps[1:2, lanes]
                    + field[EDGE + 1 : EDGE + 1 + WINDOW] * taps[2:3, lanes]
                )

            g = convolve(upg, tapg)
            v = convolve(upv, tapv)
            hidden[pl.ds(base, WINDOW), lanes] = (g / (1.0 + jnp.exp(-g)) * v).astype(BF16)

    def gate_tile(i):
        for r in range(0, tile, WINDOW):
            gate(pl.multiple_of(i * tile + r, WINDOW))

    def gate_step(i, carry):
        gate_tile(i)
        return carry

    def up_and_gate(i, carry):
        gate_tile(i - 2)
        up_tail(i)
        return carry

    up_tail(1)
    up_tail(2)
    lax.fori_loop(3, tiles - 1, up_and_gate, 0)
    lax.fori_loop(tiles - 3, tiles - 1, gate_step, 0)

    none = jnp.zeros((EDGE, wide), F32)

    @pl.when(jnp.logical_not(can_down))
    def _():
        upg[pl.ds(0, EDGE), :] = none
        upv[pl.ds(0, EDGE), :] = none

    @pl.when(jnp.logical_not(can_up))
    def _():
        upg[pl.ds(EDGE + group, EDGE), :] = none
        upv[pl.ds(EDGE + group, EDGE), :] = none

    for kind in range(2):
        pl.when(can_down)(edge_high(kind).wait_recv)
        pl.when(can_up)(edge_low(kind).wait_recv)

    gate_tile(0)
    gate_tile(tiles - 1)
    relay_all(range(3, line), downs, False)

    units = PAIR * sp

    def r_copy(k, u):
        src, dst = (
            (terms.at[u, :, :, 1 - core], near.at[u]),
            (pair_sum.at[u, 0, 1 - side], first_x.at[u]),
            (pair_sum.at[u, 1, :, 1 - row_y], first_y.at[u]),
            (sum_x.at[u], last_x.at[u]),
            (sum_y.at[u], last_y.at[u]),
        )[k]
        where = ({"tp": buddy}, {"sp": mate}, {"tp": across}, {"tp": across}, {"sp": mate})[k]
        return remote(src, dst, r_send.at[k, u], r_recv.at[k, u], **where)

    def unit_at(j):
        there, _ = step(j // (2 * PAIR))
        return there * PAIR + j // PAIR % 2, j % PAIR

    def produce(j):
        block, piece = unit_at(j)
        u = block * PAIR + piece

        @pl.when(j == 0)
        def _():
            for kind in downs:
                own_local[2 + kind].wait()

        @pl.when(j == 2 * PAIR)
        def _():
            relay_all(range(3, line), downs, True)

        @pl.when((j >= 2 * PAIR) & (piece == 0))
        def _():
            _, above = step(j // (2 * PAIR))

            @pl.when(jnp.logical_not(forwards(above)))
            def _():
                for kind in downs:
                    w_copy(kind, block, 2).wait_recv()

        @pl.when(piece == 0)
        def _():
            for i in range(group // (2 * share)):
                rows = pl.ds(i * 2 * share, 2 * share)
                term = jnp.dot(hidden[rows, :], wd[block], preferred_element_type=F32)
                term = term.astype(BF16)
                for n in range(PAIR):
                    part = term[:, n * unit : (n + 1) * unit].reshape(2, share, unit)
                    terms[block * PAIR + n, i // 2, i % 2] = part

        r_copy(0, u).start()

    def unit_of(j):
        block, piece = unit_at(j)
        return block * PAIR + piece

    def pass_first(j):
        u = unit_of(j)
        r_copy(0, u).wait_recv()
        for x in range(PAIR):
            for y in range(tp // 2):
                both = terms[u, x, y, core].astype(F32) + near[u, x, y].astype(F32)
                pair_sum[u, 0, x, y] = both[:row_half].astype(BF16)
                pair_sum[u, 1, x, y] = both[row_half:].astype(BF16)
        r_copy(1, u).start()
        r_copy(2, u).start()

    def pass_second(j):
        u = unit_of(j)
        r_copy(1, u).wait_recv()
        both = pair_sum[u, 0, side, 1 - row_y].astype(F32)
        sum_x[u] = (both + first_x[u, 1 - row_y].astype(F32)).astype(BF16)
        r_copy(3, u).start()
        r_copy(2, u).wait_recv()
        both = pair_sum[u, 1, 1 - side, row_y].astype(F32)
        sum_y[u] = (both + first_y[u, 1 - side].astype(F32)).astype(BF16)
        r_copy(4, u).start()

    lag = 6

    def down(j, carry):
        pl.when(j >= lag)(lambda: pass_second(j - lag))
        pl.when((j > 0) & (j < units + 1))(lambda: pass_first(j - 1))
        pl.when(j < units)(lambda: produce(j))
        return carry

    lax.fori_loop(0, units + lag, down, 0)

    for u in range(units):
        r_copy(3, u).wait_recv()
        r_copy(4, u).wait_recv()
        lanes = pl.ds(u * unit, unit)
        for half in range(2):
            rows = pl.ds(half * row_half, row_half)
            first = first_x[u, row_y] if half == 0 else first_y[u, side]
            last = last_x[u] if half == 0 else last_y[u]
            acc = mid[rows, lanes].astype(F32) + pair_sum[u, half, side, row_y].astype(F32)
            acc = acc + first.astype(F32) + last.astype(F32)
            out_ref[rows, lanes] = acc.astype(BF16)

    for kind in range(2 + PAIR):
        w_copy(kind, me, 2, True).wait_send()
        for block in (me, mate):
            pl.when(can_down)(w_copy(kind, block, 0).wait_send)
            pl.when(can_up)(w_copy(kind, block, 1).wait_send)

    def drain(s, carry):
        there, above = step(s)
        for kind in range(2 + PAIR):
            for other in (False, True):
                block = block_of(there, other)
                pl.when(above & can_down)(w_copy(kind, block, 0).wait_send)
                pl.when(jnp.logical_not(above) & can_up)(w_copy(kind, block, 1).wait_send)
        return carry

    lax.fori_loop(1, line, drain, 0)
    for k in range(tp - 1):
        wo_copy(k, k < 2).wait_send()
        att_copy(k).wait_send()
    for k in range(len(rows_sent)):
        n_copy(k).wait_send()
    pl.when(has_low)(kv_low.wait_send)
    pl.when(has_high)(kv_high.wait_send)
    for kind in range(2):
        pl.when(can_down)(edge_low(kind).wait_send)
        pl.when(can_up)(edge_high(kind).wait_send)

    def drain_sums(block, carry):
        for k in range(5):
            r_copy(k, block).wait_send()
        return carry

    lax.fori_loop(0, units, drain_sums, 0)


def kernel_shards(
    sp,
    tp,
    residual,
    query,
    key,
    value,
    sink,
    norm_gain,
    w_out,
    w_gate,
    w_value,
    conv_gate,
    conv_value,
    w_down,
):
    tok, width = residual.shape
    depth, hid = w_gate.shape
    cols = w_down.shape[1]
    heads = query.shape[1] // HD
    share = tok // tp
    wide = hid // PAIR
    unit = cols // PAIR
    units = PAIR * sp
    group = PAIR * tok
    inverse = THETA ** (-(np.arange(2 * HD) % (HD // 2)) * 2.0 / HD)
    local = (np.arange(tok + 2 * WINDOW) - WINDOW)[:, None] * inverse[None, :]
    first = (np.arange(sp) * tok)[:, None] * inverse[None, :]
    table = np.concatenate([np.cos(local), np.sin(local), np.cos(first), np.sin(first)])
    vmem = pl.BlockSpec(memory_space=pltpu.VMEM)
    smem = pl.BlockSpec(memory_space=pltpu.SMEM)
    anywhere = pl.BlockSpec(memory_space=pl.ANY)
    dma = pltpu.SemaphoreType.DMA
    return pl.pallas_call(
        functools.partial(layer_kernel, sp, tp),
        out_shape=pltpu.VMEM((tok // tp, width), BF16),
        in_specs=[anywhere, vmem, vmem, anywhere, smem, anywhere, vmem]
        + [anywhere] * 3
        + [vmem] * 2
        + [anywhere],
        out_specs=vmem,
        scratch_shapes=[
            pltpu.VMEM(query.shape, BF16),
            pltpu.VMEM(table.shape, F32),
            pltpu.VMEM((tok + 2 * WINDOW, 2 * HD), BF16),
            pltpu.VMEM((tok + 2 * WINDOW, 2 * HD), BF16),
            pltpu.VMEM((tok + 2 * WINDOW, 2 * HD), BF16),
            pltpu.VMEM((tok, heads * HD), BF16),
            pltpu.VMEM((tp, share, heads * HD), BF16),
            pltpu.VMEM((tp,) + w_out.shape, BF16),
            pltpu.VMEM((sp * depth, wide), BF16),
            pltpu.VMEM((sp * depth, wide), BF16),
            pltpu.VMEM((sp, wide, cols), BF16),
            pltpu.VMEM((share, width), BF16),
            pltpu.VMEM((group, width), BF16),
            pltpu.VMEM((group + 2 * EDGE, wide), F32),
            pltpu.VMEM((group + 2 * EDGE, wide), F32),
            pltpu.VMEM((group, wide), BF16),
            pltpu.VMEM((units, PAIR, tp // 2, 2, share, unit), BF16),
            pltpu.VMEM((units, PAIR, tp // 2, share, unit), BF16),
            pltpu.VMEM((units, 2, PAIR, tp // 2, share // 2, unit), BF16),
            pltpu.VMEM((units, tp // 2, share // 2, unit), BF16),
            pltpu.VMEM((units, PAIR, share // 2, unit), BF16),
            pltpu.VMEM((units, share // 2, unit), BF16),
            pltpu.VMEM((units, share // 2, unit), BF16),
            pltpu.VMEM((units, share // 2, unit), BF16),
            pltpu.VMEM((units, share // 2, unit), BF16),
            pltpu.VMEM((3, wide), F32),
            pltpu.VMEM((3, wide), F32),
            dma((8,)),
            dma((2 + PAIR, sp, 3)),
            dma((2 + PAIR, sp)),
            dma((tp - 1,)),
            dma((tp,)),
            dma((tp - 1,)),
            dma((tp,)),
            dma((2,)),
            dma((2,)),
            dma((2, 2)),
            dma((2, 2)),
            dma((9,)),
            dma((PAIR * tp, 2)),
            dma((5, units)),
            dma((5, units)),
        ],
        compiler_params=pltpu.CompilerParams(
            collective_id=0, has_side_effects=True, vmem_limit_bytes=62 * 1000 * 1000
        ),
        name="layer",
    )(
        query,
        key.T,
        value.T,
        jnp.asarray(table, F32),
        sink,
        residual,
        norm_gain.reshape(1, -1),
        w_out,
        w_gate,
        w_value,
        conv_gate,
        conv_value,
        w_down,
    )


def solution(mesh):
    sp, tp = mesh.shape["sp"], mesh.shape["tp"]

    def shards(*args):
        if args[11].shape[1] % 256 or sp % PAIR or tp != 4 or args[2].shape[1] != HD:
            return plain_shards(*args)
        return kernel_shards(sp, tp, *args)

    return jax.shard_map(
        shards,
        mesh=mesh,
        in_specs=(
            P("sp", None),
            P("sp", "tp"),
            P("sp", "tp"),
            P("sp", "tp"),
            P("tp"),
            P(),
            P("tp", None),
            P("sp", "tp"),
            P("sp", "tp"),
            P(None, "tp"),
            P(None, "tp"),
            P("tp", "sp"),
        ),
        out_specs=P(("sp", "tp"), None),
        check_vma=False,
    )
```

```python
import functools

import jax
import jax.numpy as jnp
import numpy as np
from jax import lax
from jax.experimental import pallas as pl
from jax.experimental.pallas import tpu as pltpu
from jax.sharding import PartitionSpec as P

HD = 64
WINDOW = 128


THETA = 10000.0
EPS = 1e-06


def extended(block, sides, width):
    for axis, dim in sides:
        count = lax.axis_size(axis)
        forward = [(i, i + 1) for i in range(count - 1)]
        backward = [(target, source) for source, target in forward]
        low = lax.ppermute(
            lax.slice_in_dim(block, block.shape[dim] - width, None, axis=dim), axis, forward
        )
        high = lax.ppermute(lax.slice_in_dim(block, 0, width, axis=dim), axis, backward)
        block = jnp.concatenate([low, block, high], axis=dim)
    return block


def rotate(field, positions):
    count = field.shape[0]
    parts = field.astype(jnp.float32).reshape(count, -1, HD)
    inverse = 1.0 / THETA ** (jnp.arange(0, HD, 2, dtype=jnp.float32) / HD)
    angle = positions[:, None] * inverse[None, :]
    cosine = jnp.cos(angle)[:, None, :]
    sine = jnp.sin(angle)[:, None, :]
    first = parts[..., : HD // 2]
    second = parts[..., HD // 2 :]
    turned = jnp.concatenate(
        [first * cosine - second * sine, second * cosine + first * sine], axis=-1
    )
    return turned.reshape(count, -1).astype(jnp.bfloat16)


def band_attention(queries, keys, values, sinks, start, total):
    count = queries.shape[0]
    blocks = count // WINDOW
    kv_local = keys.shape[1] // HD
    group = queries.shape[1] // (kv_local * HD)
    query_blocks = queries.reshape(blocks, WINDOW, kv_local, group, HD)
    key_band = jnp.concatenate(
        [
            keys[i * WINDOW : i * WINDOW + count].reshape(blocks, WINDOW, kv_local, HD)
            for i in range(3)
        ],
        axis=1,
    )
    value_band = jnp.concatenate(
        [
            values[i * WINDOW : i * WINDOW + count].reshape(blocks, WINDOW, kv_local, HD)
            for i in range(3)
        ],
        axis=1,
    )
    scores = jnp.einsum(
        "nqkgd,njkd->nkgqj", query_blocks, key_band, preferred_element_type=jnp.float32
    ) * HD ** (-0.5)
    block_ids = jnp.arange(blocks, dtype=jnp.int32)[:, None]
    query_pos = start + block_ids * WINDOW + jnp.arange(WINDOW, dtype=jnp.int32)[None, :]
    key_pos = start - WINDOW + block_ids * WINDOW + jnp.arange(3 * WINDOW, dtype=jnp.int32)[None, :]
    valid = (
        (key_pos[:, None, :] >= 0)
        & (key_pos[:, None, :] < total)
        & (jnp.abs(query_pos[:, :, None] - key_pos[:, None, :]) <= WINDOW)
    )
    scores = jnp.where(valid[:, None, None], scores, -1e30)
    sink_col = sinks.reshape(1, kv_local, group, 1, 1)
    top = jnp.maximum(jnp.max(scores, axis=-1, keepdims=True), sink_col)
    weights = jnp.exp(scores - top)
    denom = jnp.sum(weights, axis=-1, keepdims=True) + jnp.exp(sink_col - top)
    probs = (weights / denom).astype(jnp.bfloat16)
    out = jnp.einsum("nkgqj,njkd->nqkgd", probs, value_band, preferred_element_type=jnp.float32)
    return out.reshape(count, kv_local * group * HD).astype(jnp.bfloat16)


def rmsnorm(field, gain):
    wide = field.astype(jnp.float32)
    scale = lax.rsqrt(jnp.mean(wide * wide, axis=-1, keepdims=True) + EPS)
    return (wide * scale * gain).astype(jnp.bfloat16)


def plain_shards(
    residual,
    query,
    key,
    value,
    sink,
    norm_gain,
    w_out,
    w_gate,
    w_value,
    conv_gate,
    conv_value,
    w_down,
):
    tok_rows = query.shape[0]
    offset = lax.axis_index("sp") * tok_rows
    total = tok_rows * lax.axis_size("sp")
    share = tok_rows // lax.axis_size("tp")
    tp_index = lax.axis_index("tp")
    positions = (offset + jnp.arange(tok_rows, dtype=jnp.int32)).astype(jnp.float32)
    turned_query = rotate(query, positions)
    turned_key = rotate(key, positions)
    key_width = key.shape[1]
    band = jnp.concatenate([turned_key, value], axis=1)
    edged = extended(band, (("sp", 0),), WINDOW)
    attended = band_attention(
        turned_query, edged[:, :key_width], edged[:, key_width:], sink, offset, total
    )
    partial_value = jnp.dot(attended, w_out, preferred_element_type=jnp.float32)
    mix_full = lax.psum(partial_value.astype(jnp.bfloat16), "tp").astype(jnp.float32)
    mid_full = (residual.astype(jnp.float32) + mix_full).astype(jnp.bfloat16)
    normed = rmsnorm(mid_full, norm_gain)
    mid_rows = lax.dynamic_slice_in_dim(mid_full, tp_index * share, share, 0)
    gate_full, value_full = (
        lax.all_gather(w_gate, "sp", axis=0, tiled=True),
        lax.all_gather(w_value, "sp", axis=0, tiled=True),
    )
    gate_up = jnp.dot(normed, gate_full, preferred_element_type=jnp.float32).astype(jnp.bfloat16)
    value_up = jnp.dot(normed, value_full, preferred_element_type=jnp.float32).astype(jnp.bfloat16)
    hidden_width = gate_up.shape[1]
    stacked = jnp.concatenate([gate_up, value_up], axis=1)
    edged_up = extended(stacked, (("sp", 0),), 1).astype(jnp.float32)
    taps = jnp.concatenate([conv_gate, conv_value], axis=1).astype(jnp.float32)
    convolved = edged_up[:-2] * taps[0] + edged_up[1:-1] * taps[1] + edged_up[2:] * taps[2]
    hidden = (jax.nn.silu(convolved[:, :hidden_width]) * convolved[:, hidden_width:]).astype(
        jnp.bfloat16
    )
    terms = jnp.dot(
        hidden, lax.all_gather(w_down, "sp", axis=1, tiled=True), preferred_element_type=jnp.float32
    )
    ffn_rows = lax.psum_scatter(
        terms.astype(jnp.bfloat16), "tp", scatter_dimension=0, tiled=True
    ).astype(jnp.float32)
    return (mid_rows.astype(jnp.float32) + ffn_rows).astype(jnp.bfloat16)


F32 = jnp.float32
BF16 = jnp.bfloat16
PAIR = 2
EDGE = 8


def layer_kernel(
    sp,
    tp,
    q_ref,
    k_ref,
    v_ref,
    table_ref,
    sink_ref,
    res_ref,
    gain_ref,
    wo_ref,
    wg_ref,
    wv_ref,
    tg_ref,
    tv_ref,
    wd_ref,
    out_ref,
    q,
    table,
    band,
    key_value,
    value_key,
    att,
    att_all,
    wo,
    wg,
    wv,
    wd,
    mid,
    normed,
    upg,
    upv,
    hidden,
    terms,
    near,
    pair_sum,
    first_x,
    first_y,
    sum_x,
    sum_y,
    last_x,
    last_y,
    tapg,
    tapv,
    local_sem,
    w_send,
    w_recv,
    wo_send,
    wo_recv,
    att_send,
    att_recv,
    kv_send,
    kv_recv,
    edge_send,
    edge_recv,
    n_send,
    n_recv,
    r_send,
    r_recv,
):
    me = lax.axis_index("sp")
    my_tp = lax.axis_index("tp")
    tok = q.shape[0]
    share, width = mid.shape
    group = normed.shape[0]
    line = sp // PAIR
    place = me // PAIR
    side = me % PAIR
    mate = place * PAIR + (1 - side)
    depth = wg_ref.shape[0]
    wide = wg.shape[1]
    cols = wd_ref.shape[1]
    unit = cols // PAIR
    row_half = share // 2
    downs = tuple(range(2, 2 + PAIR))
    has_low = me > 0
    has_high = me < sp - 1
    can_down = place > 0
    can_up = place < line - 1
    end_down = place == 1
    end_up = place == line - 2
    row_y = my_tp // 2
    core = my_tp % 2
    buddy = my_tp + 1 - 2 * core
    across = lax.rem(my_tp + 2, tp)
    corner = lax.rem(buddy + 2, tp)

    def remote(src, dst, send, recv, **where):
        return pltpu.make_async_remote_copy(
            src_ref=src,
            dst_ref=dst,
            send_sem=send,
            recv_sem=recv,
            device_id=where,
            device_id_type=pl.DeviceIdType.MESH,
        )

    barrier = pltpu.get_barrier_semaphore()

    def greet(**where):
        pl.semaphore_signal(
            barrier, inc=1, device_id=where, device_id_type=pl.DeviceIdType.MESH
        )

    def own_band(i):
        lanes = pl.ds(i * WINDOW, WINDOW)
        pair = jnp.concatenate([k_ref[:, lanes], v_ref[:, lanes]], axis=0)
        band[pl.ds((i + 1) * WINDOW, WINDOW), :] = pair.astype(F32).T.astype(BF16)

    greet(sp=mate)
    for peer in (buddy, across, corner):
        greet(tp=peer)
    far_low = has_low & (side == 0)
    far_high = has_high & (side == PAIR - 1)
    pl.when(far_low)(lambda: greet(sp=me - 1))
    pl.when(far_high)(lambda: greet(sp=me + 1))
    pl.when(can_down)(lambda: greet(sp=me - PAIR))
    pl.when(can_up)(lambda: greet(sp=me + PAIR))
    count = tp
    for able in (far_low, far_high, can_down, can_up):
        count = count + jnp.where(able, 1, 0)
    early_local = [
        pltpu.make_async_copy(q_ref, q, local_sem.at[0]),
        pltpu.make_async_copy(table_ref, table, local_sem.at[3 + PAIR + 2]),
    ]
    for copy in early_local:
        copy.start()
    own_band(0)
    own_band(tok // WINDOW - 1)
    pl.semaphore_wait(barrier, count)

    def w_part(kind, half):
        start = pl.multiple_of(half * wide, wide)
        if kind > 1:
            return wd_ref.at[pl.ds(start, wide), pl.ds((kind - 2) * unit, unit)]
        return (wg_ref, wv_ref)[kind].at[:, pl.ds(start, wide)]

    def w_slot(kind, block):
        if kind > 1:
            return wd.at[block, :, pl.ds((kind - 2) * unit, unit)]
        return (wg, wv)[kind].at[pl.ds(pl.multiple_of(block * depth, depth), depth), :]

    def w_copy(kind, block, way, own=False):
        slot = w_slot(kind, block)
        src = w_part(kind, 1 - side if way == 2 else side) if own else slot
        return remote(
            src,
            slot,
            w_send.at[kind, block, way],
            w_recv.at[kind, block],
            sp=(me - PAIR, me + PAIR, mate)[way],
        )

    def step(s):
        reach = jnp.minimum(place, line - 1 - place)
        far = (s + 1) // 2
        swing = jnp.where(s % 2 == 1, place + far, place - far)
        rest = jnp.where(2 * place < line - 1, s, line - 1 - s)
        there = jnp.where(s <= 2 * reach, swing, rest)
        return there, there > place

    def forwards(above):
        return (above & can_down) | (jnp.logical_not(above) & can_up)

    def block_of(there, other, kind=0):
        if kind > 1:
            return there * PAIR + (1 if other else 0)
        return there * PAIR + (1 - side if other else side)

    def relay(s, kind, other):
        there, above = step(s)
        block = block_of(there, other, kind)

        @pl.when(forwards(above))
        def _():
            w_copy(kind, block, 2).wait_recv()
            pl.when(above & can_down)(w_copy(kind, block, 0).start)
            pl.when(jnp.logical_not(above) & can_up)(w_copy(kind, block, 1).start)

    def settle(s, kind, other):
        there, above = step(s)
        block = block_of(there, other, kind)
        pl.when(jnp.logical_not(forwards(above)))(w_copy(kind, block, 2).wait_recv)

    kv_low = remote(
        band.at[pl.ds(WINDOW, WINDOW), :],
        band.at[pl.ds(WINDOW + tok, WINDOW), :],
        kv_send.at[0],
        kv_recv.at[1],
        sp=me - 1,
    )
    kv_high = remote(
        band.at[pl.ds(tok, WINDOW), :],
        band.at[pl.ds(0, WINDOW), :],
        kv_send.at[1],
        kv_recv.at[0],
        sp=me + 1,
    )

    def shares(index, half=None):
        if half is None:
            return pl.ds(pl.multiple_of(index * share, share), share)
        size = share // 2
        return pl.ds(pl.multiple_of(index * share + half * size, size), size)

    own_local = [
        pltpu.make_async_copy(wo_ref, wo.at[my_tp], local_sem.at[1]),
        pltpu.make_async_copy(res_ref.at[shares(my_tp), :], mid, local_sem.at[2]),
    ] + [
        pltpu.make_async_copy(w_part(kind, side), w_slot(kind, me), local_sem.at[3 + kind])
        for kind in range(2 + PAIR)
    ]

    def wo_copy(k, own=True):
        slot = wo.at[my_tp if own else across]
        return remote(
            wo_ref if own else slot,
            slot,
            wo_send.at[k],
            wo_recv.at[my_tp if own else across],
            tp=(buddy, across, buddy)[k],
        )

    def arrived(ref, recv, source):
        slot = ref.at[source]
        return remote(slot, slot, wo_send.at[0], recv.at[source], tp=buddy)

    pl.when(has_low)(kv_low.start)
    pl.when(has_high)(kv_high.start)
    for copy in own_local:
        copy.start()
    for kind in range(2):
        w_copy(kind, me, 2, True).start()
        pl.when(can_down)(w_copy(kind, me, 0, True).start)
        pl.when(can_up)(w_copy(kind, me, 1, True).start)
    for kind in downs:
        w_copy(kind, me, 2, True).start()
    wo_copy(1).start()
    wo_copy(0).start()

    for ref, taps in ((tg_ref, tapg), (tv_ref, tapv)):
        taps[...] = jnp.where(side == 0, ref[:, 0:wide], ref[:, wide : 2 * wide]).astype(F32)

    blank = jnp.zeros((WINDOW, band.shape[1]), BF16)

    @pl.when(jnp.logical_not(has_low))
    def _():
        band[pl.ds(0, WINDOW), :] = blank

    @pl.when(jnp.logical_not(has_high))
    def _():
        band[pl.ds(WINDOW + tok, WINDOW), :] = blank

    for i in range(1, tok // WINDOW - 1):
        own_band(i)
    for copy in early_local:
        copy.wait()
    pl.when(has_low)(kv_high.wait_recv)
    pl.when(has_high)(kv_low.wait_recv)
    heads = q.shape[1] // HD
    span = 3 * WINDOW
    steps = tok + 2 * WINDOW
    total = tok * sp
    lane = lax.broadcasted_iota(jnp.int32, (WINDOW, 2 * HD), 1)
    early = lane % HD < HD // 2
    low = lane < HD

    def turn(field, start):
        rows = pl.ds(start, WINDOW)
        base_cos = table[pl.ds(2 * steps + me, 1), :]
        base_sin = table[pl.ds(2 * steps + sp + me, 1), :]
        near_cos = table[rows, :]
        near_sin = table[pl.ds(pl.multiple_of(steps + start, WINDOW), WINDOW), :]
        cosine = base_cos * near_cos - base_sin * near_sin
        sine = base_sin * near_cos + base_cos * near_sin
        ahead = pltpu.roll(field, 2 * HD - HD // 2, 1)
        behind = pltpu.roll(field, HD // 2, 1)
        return field * cosine + jnp.where(early, -ahead, behind) * sine

    def turn_keys(i, carry):
        start = pl.multiple_of(i * WINDOW, WINDOW)
        field = band[pl.ds(start, WINDOW), :].astype(F32)
        field = jnp.where(low, turn(field, start), field)
        key_value[pl.ds(start, WINDOW), :] = field.astype(BF16)
        value_key[pl.ds(start, WINDOW), :] = pltpu.roll(field, HD, 1).astype(BF16)
        return carry

    lax.fori_loop(0, tok // WINDOW + 2, turn_keys, 0)

    def att_copy(k):
        peer = (corner, across, buddy)[k]
        return remote(
            att.at[shares(peer), :],
            att_all.at[my_tp],
            att_send.at[k],
            att_recv.at[my_tp],
            tp=peer,
        )

    per = share // WINDOW

    def attend(i, carry):
        k = i // per
        target = jnp.where(
            k == 0, corner, jnp.where(k == 1, across, jnp.where(k == 2, buddy, my_tp))
        )
        start = pl.multiple_of(target * share + i % per * WINDOW, WINDOW)
        straight = key_value[pl.ds(start, span), :]
        crossed = value_key[pl.ds(start, span), :]
        row = lax.broadcasted_iota(jnp.int32, (WINDOW, span), 0)
        col = lax.broadcasted_iota(jnp.int32, (WINDOW, span), 1)
        key_pos = col + (me * tok - WINDOW + start)
        valid = (col >= row) & (col <= row + 2 * WINDOW) & (key_pos >= 0) & (key_pos < total)

        def head(query, sink, keys, values):
            scores = lax.dot_general(
                query, keys, (((1,), (1,)), ((), ())), preferred_element_type=F32
            )
            scores = jnp.where(valid, scores, -1e30)
            top = jnp.maximum(jnp.max(scores, axis=-1, keepdims=True), sink)
            weights = jnp.exp(scores - top)
            denom = jnp.sum(weights, axis=-1, keepdims=True) + jnp.exp(sink - top)
            probs = (weights * (1.0 / denom)).astype(BF16)
            return jnp.dot(probs, values, preferred_element_type=F32)

        for h in range(0, heads, 2):
            lanes = pl.ds(h * HD, 2 * HD)
            field = q[pl.ds(start, WINDOW), lanes].astype(F32)
            field = turn(field, pl.multiple_of(start + WINDOW, WINDOW)) * HD**-0.5
            even = head(
                jnp.where(low, field, 0.0).astype(BF16), sink_ref[h], straight, crossed
            )
            odd = head(
                jnp.where(low, 0.0, field).astype(BF16), sink_ref[h + 1], crossed, straight
            )
            att[pl.ds(start, WINDOW), lanes] = jnp.where(low, even, odd).astype(BF16)
        for n in range(tp - 1):
            pl.when(i == per * (n + 1) - 1)(att_copy(n).start)

        @pl.when(i == per * 2 - 1)
        def _():
            for kind in range(2):
                w_copy(kind, mate, 2).wait_recv()
                pl.when(can_down)(w_copy(kind, mate, 0).start)
                pl.when(can_up)(w_copy(kind, mate, 1).start)
            for kind in range(2):
                for s in (1, 2):
                    if s < line:
                        relay(s, kind, False)

        return carry

    lax.fori_loop(0, tok // WINDOW, attend, 0)
    att_all[my_tp] = att[shares(my_tp), :]
    for kind in range(2):
        for s in (1, 2):
            if s < line:
                relay(s, kind, True)
    arrived(wo, wo_recv, across).wait_recv()
    wo_copy(2, False).start()

    own_local[0].wait()
    own_local[1].wait()
    for source in (buddy, across, corner):
        if source is not across:
            arrived(wo, wo_recv, source).wait_recv()
        arrived(att_all, att_recv, source).wait_recv()
    piece = 512
    mine = side * tp + my_tp
    squares = jnp.zeros((share, 1), F32)
    for c in range(0, width, piece):
        acc = jnp.zeros((share, piece), F32)
        for k in range(tp):
            term = jnp.dot(att_all[k], wo[k, :, pl.ds(c, piece)], preferred_element_type=F32)
            acc = acc + term.astype(BF16).astype(F32)
        new = (mid[:, pl.ds(c, piece)].astype(F32) + acc).astype(BF16)
        mid[:, pl.ds(c, piece)] = new
        field = new.astype(F32)
        squares = squares + jnp.sum(field * field, axis=-1, keepdims=True)
    scale = lax.rsqrt(squares * (1.0 / width) + EPS)
    for c in range(0, width, piece):
        field = mid[:, pl.ds(c, piece)].astype(F32)
        normed[shares(mine), pl.ds(c, piece)] = (
            field * scale * gain_ref[:, pl.ds(c, piece)]
        ).astype(BF16)

    from_mate = (1 - side) * tp + my_tp
    from_across = side * tp + across
    from_corner = side * tp + corner
    diagonal = (1 - side) * tp + across
    rows_sent = [
        (mine, None, "buddy"),
        (mine, None, "mate"),
        (mine, None, "across"),
        (from_mate, None, "buddy"),
        (from_mate, 0, "across"),
        (from_across, None, "buddy"),
        (from_across, 1, "mate"),
        (diagonal, 0, "buddy"),
        (diagonal, 1, "buddy"),
    ]

    def n_copy(k):
        index, half, goal = rows_sent[k]
        slot = normed.at[shares(index, half), :]
        where = {"sp": mate} if goal == "mate" else {"tp": buddy if goal == "buddy" else across}
        return remote(slot, slot, n_send.at[k], n_recv.at[index, half or 0], **where)

    def n_wait(index, half=None):
        slot = normed.at[shares(index, half), :]
        remote(slot, slot, n_send.at[0], n_recv.at[index, half or 0], tp=buddy).wait_recv()

    for k in (1, 2, 0):
        n_copy(k).start()

    def relay_all(steps, kinds, other):
        for s in steps:
            if s < line:
                for kind in kinds:
                    relay(s, kind, other)

    relay_all(range(3, line), (0, 1), False)
    relay_all(range(3, line), (0, 1), True)

    for kind in downs:
        w_copy(kind, mate, 2).wait_recv()
    inner_down = can_down & jnp.logical_not(end_down)
    inner_up = can_up & jnp.logical_not(end_up)

    def start_down(down, up, x):
        for kind in downs:
            for own in (True, False):
                here = (side == x) if own else (side != x)
                block = me if own else mate
                pl.when(down & here)(w_copy(kind, block, 0, own).start)
                pl.when(up & here)(w_copy(kind, block, 1, own).start)

    start_down(can_down, can_up, 0)
    start_down(inner_down, inner_up, 1)

    last_there, _ = step(line - 1)
    plane = PAIR * depth
    tail = pl.ds(pl.multiple_of(last_there * plane, plane), plane)
    main_start = jnp.where(last_there == 0, plane, 0)
    main = pl.ds(pl.multiple_of(main_start, plane), (line - 1) * plane)
    tile = share
    tiles = group // tile

    def up_main(i):
        left = normed[shares(i), main]
        rows = pl.ds(pl.multiple_of(i * tile + EDGE, EDGE), tile)
        for weight, dest in ((wg, upg), (wv, upv)):
            dest[rows, :] = jnp.dot(left, weight[main, :], preferred_element_type=F32)

    def up_tail(i):
        left = normed[shares(i), tail]
        rows = pl.ds(pl.multiple_of(i * tile + EDGE, EDGE), tile)
        for weight, dest in ((wg, upg), (wv, upv)):
            term = jnp.dot(left, weight[tail, :], preferred_element_type=F32)
            dest[rows, :] = (dest[rows, :] + term).astype(BF16).astype(F32)

    def settle_up(s):
        for other in (False, True):
            for kind in range(2):
                settle(s, kind, other)

    n_wait(from_mate)
    n_copy(4).start()
    n_copy(3).start()
    n_wait(from_across)
    n_copy(6).start()
    n_copy(5).start()
    for s in range(1, line - 1):
        settle_up(s)
    for kind in range(2):
        own_local[2 + kind].wait()
    up_main(mine)
    n_wait(side * tp + buddy)
    up_main(side * tp + buddy)
    up_main(from_mate)
    up_main(from_across)
    n_wait((1 - side) * tp + buddy)
    up_main((1 - side) * tp + buddy)
    n_wait(from_corner)
    up_main(from_corner)
    for half in range(2):
        n_wait(diagonal, half)
        n_copy(7 + half).start()
    up_main(diagonal)
    for half in range(2):
        n_wait((1 - side) * tp + corner, half)
    up_main((1 - side) * tp + corner)
    settle_up(line - 1)

    def up_step(i, carry):
        up_tail(i)
        return carry

    def edge_low(kind):
        ref = (upg, upv)[kind]
        return remote(
            ref.at[pl.ds(EDGE, EDGE), :],
            ref.at[pl.ds(EDGE + group, EDGE), :],
            edge_send.at[0, kind],
            edge_recv.at[1, kind],
            sp=me - PAIR,
        )

    def edge_high(kind):
        ref = (upg, upv)[kind]
        return remote(
            ref.at[pl.ds(group, EDGE), :],
            ref.at[pl.ds(0, EDGE), :],
            edge_send.at[1, kind],
            edge_recv.at[0, kind],
            sp=me + PAIR,
        )

    up_tail(0)
    up_tail(tiles - 1)
    for kind in range(2):
        pl.when(can_down)(edge_low(kind).start)
        pl.when(can_up)(edge_high(kind).start)
    start_down(can_down & end_down, can_up & end_up, 1)
    for s in (1, 2):
        for other in (False, True):
            relay_all((s,), downs, other)

    def gate(base):
        for c in range(0, wide, 256):
            lanes = pl.ds(c, 256)

            def convolve(ref, taps):
                field = ref[pl.ds(base, WINDOW + 2 * EDGE), lanes]
                return (
                    field[EDGE - 1 : EDGE - 1 + WINDOW] * taps[0:1, lanes]
                    + field[EDGE : EDGE + WINDOW] * taps[1:2, lanes]
                    + field[EDGE + 1 : EDGE + 1 + WINDOW] * taps[2:3, lanes]
                )

            g = convolve(upg, tapg)
            v = convolve(upv, tapv)
            hidden[pl.ds(base, WINDOW), lanes] = (g / (1.0 + jnp.exp(-g)) * v).astype(BF16)

    def gate_tile(i):
        for r in range(0, tile, WINDOW):
            gate(pl.multiple_of(i * tile + r, WINDOW))

    def gate_step(i, carry):
        gate_tile(i)
        return carry

    def up_and_gate(i, carry):
        gate_tile(i - 2)
        up_tail(i)
        return carry

    up_tail(1)
    up_tail(2)
    lax.fori_loop(3, tiles - 1, up_and_gate, 0)
    lax.fori_loop(tiles - 3, tiles - 1, gate_step, 0)

    none = jnp.zeros((EDGE, wide), F32)

    @pl.when(jnp.logical_not(can_down))
    def _():
        upg[pl.ds(0, EDGE), :] = none
        upv[pl.ds(0, EDGE), :] = none

    @pl.when(jnp.logical_not(can_up))
    def _():
        upg[pl.ds(EDGE + group, EDGE), :] = none
        upv[pl.ds(EDGE + group, EDGE), :] = none

    for kind in range(2):
        pl.when(can_down)(edge_high(kind).wait_recv)
        pl.when(can_up)(edge_low(kind).wait_recv)

    gate_tile(0)
    gate_tile(tiles - 1)
    relay_all(range(3, line), downs, False)

    units = PAIR * sp

    def r_copy(k, u):
        src, dst = (
            (terms.at[u, :, :, 1 - core], near.at[u]),
            (pair_sum.at[u, 0, 1 - side], first_x.at[u]),
            (pair_sum.at[u, 1, :, 1 - row_y], first_y.at[u]),
            (sum_x.at[u], last_x.at[u]),
            (sum_y.at[u], last_y.at[u]),
        )[k]
        where = ({"tp": buddy}, {"sp": mate}, {"tp": across}, {"tp": across}, {"sp": mate})[k]
        return remote(src, dst, r_send.at[k, u], r_recv.at[k, u], **where)

    def unit_at(j):
        there, _ = step(j // (2 * PAIR))
        return there * PAIR + j // PAIR % 2, j % PAIR

    def produce(j):
        block, piece = unit_at(j)
        u = block * PAIR + piece

        @pl.when(j == 0)
        def _():
            for kind in downs:
                own_local[2 + kind].wait()

        @pl.when(j == 2 * PAIR)
        def _():
            relay_all(range(3, line), downs, True)

        @pl.when((j >= 2 * PAIR) & (piece == 0))
        def _():
            _, above = step(j // (2 * PAIR))

            @pl.when(jnp.logical_not(forwards(above)))
            def _():
                for kind in downs:
                    w_copy(kind, block, 2).wait_recv()

        @pl.when(piece == 0)
        def _():
            for i in range(group // (2 * share)):
                rows = pl.ds(i * 2 * share, 2 * share)
                term = jnp.dot(hidden[rows, :], wd[block], preferred_element_type=F32)
                term = term.astype(BF16)
                for n in range(PAIR):
                    part = term[:, n * unit : (n + 1) * unit].reshape(2, share, unit)
                    terms[block * PAIR + n, i // 2, i % 2] = part

        r_copy(0, u).start()

    def unit_of(j):
        block, piece = unit_at(j)
        return block * PAIR + piece

    def pass_first(j):
        u = unit_of(j)
        r_copy(0, u).wait_recv()
        for x in range(PAIR):
            for y in range(tp // 2):
                both = terms[u, x, y, core].astype(F32) + near[u, x, y].astype(F32)
                pair_sum[u, 0, x, y] = both[:row_half].astype(BF16)
                pair_sum[u, 1, x, y] = both[row_half:].astype(BF16)
        r_copy(1, u).start()
        r_copy(2, u).start()

    def pass_second(j):
        u = unit_of(j)
        r_copy(1, u).wait_recv()
        both = pair_sum[u, 0, side, 1 - row_y].astype(F32)
        sum_x[u] = (both + first_x[u, 1 - row_y].astype(F32)).astype(BF16)
        r_copy(3, u).start()
        r_copy(2, u).wait_recv()
        both = pair_sum[u, 1, 1 - side, row_y].astype(F32)
        sum_y[u] = (both + first_y[u, 1 - side].astype(F32)).astype(BF16)
        r_copy(4, u).start()

    lag = 6

    def down(j, carry):
        pl.when(j >= lag)(lambda: pass_second(j - lag))
        pl.when((j > 0) & (j < units + 1))(lambda: pass_first(j - 1))
        pl.when(j < units)(lambda: produce(j))
        return carry

    lax.fori_loop(0, units + lag, down, 0)

    for u in range(units):
        r_copy(3, u).wait_recv()
        r_copy(4, u).wait_recv()
        lanes = pl.ds(u * unit, unit)
        for half in range(2):
            rows = pl.ds(half * row_half, row_half)
            first = first_x[u, row_y] if half == 0 else first_y[u, side]
            last = last_x[u] if half == 0 else last_y[u]
            acc = mid[rows, lanes].astype(F32) + pair_sum[u, half, side, row_y].astype(F32)
            acc = acc + first.astype(F32) + last.astype(F32)
            out_ref[rows, lanes] = acc.astype(BF16)

    for kind in range(2 + PAIR):
        w_copy(kind, me, 2, True).wait_send()
        for block in (me, mate):
            pl.when(can_down)(w_copy(kind, block, 0).wait_send)
            pl.when(can_up)(w_copy(kind, block, 1).wait_send)

    def drain(s, carry):
        there, above = step(s)
        for kind in range(2 + PAIR):
            for other in (False, True):
                block = block_of(there, other)
                pl.when(above & can_down)(w_copy(kind, block, 0).wait_send)
                pl.when(jnp.logical_not(above) & can_up)(w_copy(kind, block, 1).wait_send)
        return carry

    lax.fori_loop(1, line, drain, 0)
    for k in range(tp - 1):
        wo_copy(k, k < 2).wait_send()
        att_copy(k).wait_send()
    for k in range(len(rows_sent)):
        n_copy(k).wait_send()
    pl.when(has_low)(kv_low.wait_send)
    pl.when(has_high)(kv_high.wait_send)
    for kind in range(2):
        pl.when(can_down)(edge_low(kind).wait_send)
        pl.when(can_up)(edge_high(kind).wait_send)

    def drain_sums(block, carry):
        for k in range(5):
            r_copy(k, block).wait_send()
        return carry

    lax.fori_loop(0, units, drain_sums, 0)


def kernel_shards(
    sp,
    tp,
    residual,
    query,
    key,
    value,
    sink,
    norm_gain,
    w_out,
    w_gate,
    w_value,
    conv_gate,
    conv_value,
    w_down,
):
    tok, width = residual.shape
    depth, hid = w_gate.shape
    cols = w_down.shape[1]
    heads = query.shape[1] // HD
    share = tok // tp
    wide = hid // PAIR
    unit = cols // PAIR
    units = PAIR * sp
    group = PAIR * tok
    inverse = THETA ** (-(np.arange(2 * HD) % (HD // 2)) * 2.0 / HD)
    local = (np.arange(tok + 2 * WINDOW) - WINDOW)[:, None] * inverse[None, :]
    first = (np.arange(sp) * tok)[:, None] * inverse[None, :]
    table = np.concatenate([np.cos(local), np.sin(local), np.cos(first), np.sin(first)])
    vmem = pl.BlockSpec(memory_space=pltpu.VMEM)
    smem = pl.BlockSpec(memory_space=pltpu.SMEM)
    anywhere = pl.BlockSpec(memory_space=pl.ANY)
    dma = pltpu.SemaphoreType.DMA
    return pl.pallas_call(
        functools.partial(layer_kernel, sp, tp),
        out_shape=pltpu.VMEM((tok // tp, width), BF16),
        in_specs=[anywhere, vmem, vmem, anywhere, smem, anywhere, vmem]
        + [anywhere] * 3
        + [vmem] * 2
        + [anywhere],
        out_specs=vmem,
        scratch_shapes=[
            pltpu.VMEM(query.shape, BF16),
            pltpu.VMEM(table.shape, F32),
            pltpu.VMEM((tok + 2 * WINDOW, 2 * HD), BF16),
            pltpu.VMEM((tok + 2 * WINDOW, 2 * HD), BF16),
            pltpu.VMEM((tok + 2 * WINDOW, 2 * HD), BF16),
            pltpu.VMEM((tok, heads * HD), BF16),
            pltpu.VMEM((tp, share, heads * HD), BF16),
            pltpu.VMEM((tp,) + w_out.shape, BF16),
            pltpu.VMEM((sp * depth, wide), BF16),
            pltpu.VMEM((sp * depth, wide), BF16),
            pltpu.VMEM((sp, wide, cols), BF16),
            pltpu.VMEM((share, width), BF16),
            pltpu.VMEM((group, width), BF16),
            pltpu.VMEM((group + 2 * EDGE, wide), F32),
            pltpu.VMEM((group + 2 * EDGE, wide), F32),
            pltpu.VMEM((group, wide), BF16),
            pltpu.VMEM((units, PAIR, tp // 2, 2, share, unit), BF16),
            pltpu.VMEM((units, PAIR, tp // 2, share, unit), BF16),
            pltpu.VMEM((units, 2, PAIR, tp // 2, share // 2, unit), BF16),
            pltpu.VMEM((units, tp // 2, share // 2, unit), BF16),
            pltpu.VMEM((units, PAIR, share // 2, unit), BF16),
            pltpu.VMEM((units, share // 2, unit), BF16),
            pltpu.VMEM((units, share // 2, unit), BF16),
            pltpu.VMEM((units, share // 2, unit), BF16),
            pltpu.VMEM((units, share // 2, unit), BF16),
            pltpu.VMEM((3, wide), F32),
            pltpu.VMEM((3, wide), F32),
            dma((8,)),
            dma((2 + PAIR, sp, 3)),
            dma((2 + PAIR, sp)),
            dma((tp - 1,)),
            dma((tp,)),
            dma((tp - 1,)),
            dma((tp,)),
            dma((2,)),
            dma((2,)),
            dma((2, 2)),
            dma((2, 2)),
            dma((9,)),
            dma((PAIR * tp, 2)),
            dma((5, units)),
            dma((5, units)),
        ],
        compiler_params=pltpu.CompilerParams(
            collective_id=0, has_side_effects=True, vmem_limit_bytes=62 * 1000 * 1000
        ),
        name="layer",
    )(
        query,
        key.T,
        value.T,
        jnp.asarray(table, F32),
        sink,
        residual,
        norm_gain.reshape(1, -1),
        w_out,
        w_gate,
        w_value,
        conv_gate,
        conv_value,
        w_down,
    )


def solution(mesh):
    sp, tp = mesh.shape["sp"], mesh.shape["tp"]

    def shards(*args):
        if args[11].shape[1] % 256 or sp % PAIR or tp != 4 or args[2].shape[1] != HD:
            return plain_shards(*args)
        return kernel_shards(sp, tp, *args)

    return jax.shard_map(
        shards,
        mesh=mesh,
        in_specs=(
            P("sp", None),
            P("sp", "tp"),
            P("sp", "tp"),
            P("sp", "tp"),
            P("tp"),
            P(),
            P("tp", None),
            P("sp", "tp"),
            P("sp", "tp"),
            P(None, "tp"),
            P(None, "tp"),
            P("tp", "sp"),
        ),
        out_specs=P(("sp", "tp"), None),
        check_vma=False,
    )
```
